256 devices in a mesh: ep: 64 (over z, x, core), tp: 4 (over y).
Axes of the slice: x: 4, y: 4, z: 8, core: 2. Of those that a mesh axis runs over, the one named last changes fastest.
Arguments:
- memory_query_matrix: bfloat16 [32768, 1024], P('ep', 'tp'), may hold values from -0.59765625 to 2
- memory_key_matrix: bfloat16 [32768, 1024], P('ep', 'tp'), may hold values from -0.59765625 to 2
- memory_value_matrix: bfloat16 [32768, 1024], P('ep', 'tp'), may hold values from -6 to 6
- input_gate_logits: float32 [4, 32768], P('tp', 'ep'), may hold values from -6 to 260
- forget_gate_logits: float32 [4, 32768], P('tp', 'ep'), may hold values from -1 to 20
- forget_log_boosts: float32 [4, 32768], P('tp', 'ep'), may hold values from -0.7 to 0
- head_norm_scale: float32 [1024], P('tp'), may hold values from 0.1 to 1.9
- memory_output_matrix: bfloat16 [1024, 2048], replicated, may hold values from -0.1875 to 0.1875
- projection_norm_scale: float32 [2048], replicated, may hold values from 0.1 to 1.9
- second_batch_rows: bfloat16 [49152, 2048], P(('ep', 'tp')), may hold values from -6 to 6
- expert_prenorm_scale: float32 [2048], replicated, may hold values from 0.1 to 1.9
- selected_expert_index: int32 [49152, 2], P(('ep', 'tp')), may hold values from 0 to 63, all different within a row; in each aligned block of 192 rows (0 to 191, 192 to 383, ...) at most 12 rows name the same one
- group_route_probability: float32 [49152], P(('ep', 'tp')), may hold values from 0.2 to 1
- expert_choice_scores: float32 [49152, 2], P(('ep', 'tp')), may hold values from -6 to 6
- expert_gate_matrix: bfloat16 [64, 2048, 512], P('ep'), may hold values from -0.125 to 0.125
- expert_up_matrix: bfloat16 [64, 2048, 512], P('ep'), may hold values from -0.125 to 0.125
- expert_down_matrix: bfloat16 [64, 512, 2048], P('ep'), may hold values from -0.25 to 0.25
Outputs:
- mixed_rows: bfloat16 [32768, 2048], P(('ep', 'tp'))
- routed_rows: bfloat16 [49152, 2048], P(('ep', 'tp'))
The draws below stay inside these ranges and needn't reach their ends.
Inputs may be any that keep to these rules, and one draw needn't show every extreme that they name: `selected_expert_index`: each row names 2 different experts; among the rows of one device no expert is named more than 12 times, and in some device one expert is named exactly that often.
All inputs are finite; a program needn't handle non-finite values.
Results may differ from the reference program's by a relative error of at most 0.013.
Values may be sent and summed in bfloat16 or wider, within the bound.
A program may use at most 128 MiB of HBM per device.

```python
import math
import jax
import jax.numpy as jnp
import numpy as np
from jax import lax

D = 2048
HEADS = 4
HEAD_SIZE = 256
CELL_WIDTH = 1024
SPAN = 128
MIX_DEV = 512
SEQ_LEN = 32768
EXPERT_HIDDEN = 512
TOPK = 2
ROUTED_DEV = 192
ROUTED = 49152
EXPERTS = 64
CAPACITY = 12


def draw_forget_gate_logits(key, part):
    keys = jax.random.split(jax.random.fold_in(key, 71), 3)
    order = jax.random.permutation(keys[0], HEADS)
    quick = HEADS // 2
    slow_bias = math.log(SEQ_LEN) + 0.6
    bias = jnp.where(order < quick, 4.2, slow_bias).astype(jnp.float32)
    pieces = SEQ_LEN // MIX_DEV
    offset = jax.random.uniform(keys[1], (HEADS, pieces, 1), jnp.float32, -0.7, 0.7)
    offset = jnp.broadcast_to(offset, (HEADS, pieces, MIX_DEV)).reshape(HEADS, SEQ_LEN)
    noise = jnp.clip(jax.random.normal(keys[2], (HEADS, SEQ_LEN), jnp.float32), -4.0, 4.0)
    return bias[:, None] + offset + noise


def draw_forget_log_boosts(key, part):
    keys = jax.random.split(jax.random.fold_in(key, 83), 2)
    spots = jax.random.randint(keys[0], (HEADS, 3), 0, SEQ_LEN)
    depth = jax.random.uniform(keys[1], (HEADS, 3), jnp.float32, -0.69, -0.22)
    places = jnp.arange(SEQ_LEN, dtype=jnp.int32)
    hits = places[None, None, :] == spots[:, :, None]
    return jnp.min(jnp.where(hits, depth[:, :, None], 0.0), axis=1)


def draw_input_gate_logits(key, part):
    keys = jax.random.split(jax.random.fold_in(key, 97), 1)
    return jnp.clip(jax.random.normal(keys[0], (HEADS, SEQ_LEN), jnp.float32), -6.0, 6.0)


def shard_levels(stream_key, dims, shards, least, high):
    def one(dim, shards_of):
        heights = jax.random.uniform(jax.random.fold_in(jax.random.fold_in(stream_key, 6), dim), (shards_of,), jnp.float32, least / len(shards), high / len(shards))
        return jnp.repeat(jnp.exp(heights), dims[dim] // shards_of).reshape((-1,) + (1,) * (len(dims) - dim - 1))

    loudness = one(*shards[0])
    for cut in shards[1:]:
        loudness = loudness * one(*cut)
    return loudness


def shared_out(own_key, own, number, rows, count, top, most, skew):
    order = jax.random.permutation(own_key, count)
    packed, ordinary = portions_of(count, rows * top, most, skew, True), portions_of(count, rows * top, most, skew, False)
    places = jnp.arange(count)

    def named(sizes, turn):
        used = int((sizes > 0).sum())
        fixed = max(1, used // 4)
        passed = fixed + (places - fixed + turn * (used - fixed)) % max(1, count - fixed)
        return jnp.zeros((count,), jnp.int32).at[order[jnp.where(places < fixed, places, passed)]].set(jnp.asarray(sizes, jnp.int32))

    sizes = jnp.where(number % 4 == 0, named(packed, number // 4), named(ordinary, number - number // 4 - 1))
    mixed = jax.random.permutation(jax.random.fold_in(own, 3), count)
    giver, sink = mixed[0:count // 2 * 2:2], mixed[1:count // 2 * 2:2]
    slack = jnp.minimum(sizes[giver] - 1, most - sizes[sink]) // 2
    slack = jnp.where((giver == order[0]) | (sink == order[0]) | (sizes[sink] == 0), 0, jnp.maximum(slack, 0))
    passed = jax.random.randint(jax.random.fold_in(own, 4), (count // 2,), 0, 1 << 20) % (slack + 1)
    sizes = sizes.at[giver].add(-passed).at[sink].add(passed)
    items = jnp.searchsorted(jnp.cumsum(sizes), jnp.arange(rows * top), side="right").astype(jnp.int32)
    table = items.reshape(top, rows).T
    table = table[jax.random.permutation(jax.random.fold_in(own, 1), rows)]
    turn = jax.random.randint(jax.random.fold_in(own, 2), (rows, 1), 0, top)
    return jnp.take_along_axis(table, (jnp.arange(top)[None, :] + turn) % top, axis=1)


def portions_of(count, total, most, lean, full):
    portions = [(1 << 20) // math.isqrt(standing ** lean) + 1 for standing in range(1, count + 1)]
    largest = most if full else min(most, max(-(-total // count), total * portions[0] // sum(portions)))
    least = 1 if total - largest >= count - 1 else 0
    given, surplus = [largest] + [least] * (count - 1), total - largest - least * (count - 1)
    while surplus > 0:
        free = [i for i in range(1, count) if given[i] < largest] or [i for i in range(1, count) if given[i] < most]
        mass, left = sum([portions[i] for i in free]), surplus
        for i in free:
            extra = min(most - given[i], max(1, left * portions[i] // mass), surplus)
            given[i] = given[i] + extra
            surplus = surplus - extra
    return np.array(given)


def bell_draw(own_key, dims, deviation, limit, cuts=(), held_as=jnp.bfloat16):
    array = deviation * jax.random.normal(own_key, dims, jnp.float32)
    if cuts:
        array = array * shard_levels(own_key, dims, cuts, -0.22, 0.18)
    return jnp.clip(array, -limit, limit).astype(held_as)


def setup_inputs(seed: int = 0) -> dict:
    key_of = jax.random.split(jax.random.key(seed), 18)
    memory_query_matrix = jnp.clip(-0.59765625 + 2.5976562 * jax.random.uniform(key_of[0], (SEQ_LEN, CELL_WIDTH), jnp.float32) ** shard_levels(key_of[0], (SEQ_LEN, CELL_WIDTH), ((0, 64), (1, 4)), -0.2, 0.2), -0.59765625, 2.0).astype(jnp.bfloat16)
    memory_key_matrix = jnp.clip(-0.59765625 + 2.5976562 * jax.random.uniform(key_of[1], (SEQ_LEN, CELL_WIDTH), jnp.float32) ** shard_levels(key_of[1], (SEQ_LEN, CELL_WIDTH), ((0, 64), (1, 4)), -0.2, 0.2), -0.59765625, 2.0).astype(jnp.bfloat16)
    memory_value_matrix = bell_draw(key_of[2], (SEQ_LEN, CELL_WIDTH), 1.0, 6.0, ((0, 64), (1, 4)))
    input_gate_logits = draw_input_gate_logits(jax.random.fold_in(key_of[17], 71), 0)
    forget_gate_logits = draw_forget_gate_logits(jax.random.fold_in(key_of[17], 71), 0)
    forget_log_boosts = draw_forget_log_boosts(jax.random.fold_in(key_of[17], 71), 0)
    head_norm_scale = jnp.clip(1.0 + 0.18 * jax.random.normal(key_of[6], (CELL_WIDTH,), jnp.float32), 0.1, 1.9)
    memory_output_matrix = bell_draw(key_of[7], (CELL_WIDTH, D), CELL_WIDTH ** -0.5, 0.1875)
    projection_norm_scale = jnp.clip(1.0 + 0.18 * jax.random.normal(key_of[8], (D,), jnp.float32), 0.1, 1.9)
    second_batch_rows = bell_draw(key_of[9], (ROUTED, D), 1.0, 6.0, ((0, 256),))
    expert_prenorm_scale = jnp.clip(1.0 + 0.18 * jax.random.normal(key_of[10], (D,), jnp.float32), 0.1, 1.9)
    selected_expert_index_keys = jax.random.split(jax.random.fold_in(key_of[11], 1), ROUTED // ROUTED_DEV)
    selected_expert_index_turns = jax.random.permutation(jax.random.fold_in(key_of[11], 3), ROUTED // ROUTED_DEV)
    selected_expert_index = jax.vmap(lambda own, number: shared_out(jax.random.fold_in(key_of[11], 2), own, number, ROUTED_DEV, EXPERTS, TOPK, CAPACITY, 1))(selected_expert_index_keys, selected_expert_index_turns).reshape((ROUTED, TOPK))
    group_route_probability = jnp.clip(0.2 + 0.8 * jax.random.uniform(key_of[12], (ROUTED,), jnp.float32) ** shard_levels(key_of[12], (ROUTED,), ((0, 256),), -0.2, 0.2), 0.2, 1.0)
    expert_choice_scores = bell_draw(key_of[13], (ROUTED, TOPK), 1.5, 6.0, ((0, 256),), jnp.float32)
    expert_gate_matrix = bell_draw(key_of[14], (EXPERTS, D, EXPERT_HIDDEN), D ** -0.5, 0.125, ((0, 64),))
    expert_up_matrix = bell_draw(key_of[15], (EXPERTS, D, EXPERT_HIDDEN), D ** -0.5, 0.125, ((0, 64),))
    expert_down_matrix = bell_draw(key_of[16], (EXPERTS, EXPERT_HIDDEN, D), EXPERT_HIDDEN ** -0.5, 0.25, ((0, 64),))
    return dict(memory_query_matrix=memory_query_matrix, memory_key_matrix=memory_key_matrix, memory_value_matrix=memory_value_matrix, input_gate_logits=input_gate_logits, forget_gate_logits=forget_gate_logits, forget_log_boosts=forget_log_boosts, head_norm_scale=head_norm_scale, memory_output_matrix=memory_output_matrix, projection_norm_scale=projection_norm_scale, second_batch_rows=second_batch_rows, expert_prenorm_scale=expert_prenorm_scale, selected_expert_index=selected_expert_index, group_route_probability=group_route_probability, expert_choice_scores=expert_choice_scores, expert_gate_matrix=expert_gate_matrix, expert_up_matrix=expert_up_matrix, expert_down_matrix=expert_down_matrix)


floor_log = -1e+30
norm_eps = 1e-06
exact = lax.Precision.HIGHEST

def rms_scale(values, gain):
    squares = lax.optimization_barrier(jnp.mean(values * values, axis=-1, keepdims=True))
    return values * lax.rsqrt(squares + norm_eps) * gain

def span_step(carry, inputs):
    memory, normer, stabil = carry
    query, keyrow, valrow, in_gate, log_retain_factor = inputs
    key_scale = query.shape[-1] ** (-0.5)
    length = query.shape[1]
    causal = jnp.tril(jnp.ones((length, length), dtype=bool))
    cumulative = jnp.cumsum(log_retain_factor, axis=-1)
    decay_map = cumulative[:, :, None] - cumulative[:, None, :] + in_gate[:, None, :]
    decay_map = jnp.where(causal[None], decay_map, -jnp.inf)
    carried = cumulative + stabil[:, None]
    peak = jnp.maximum(carried, lax.optimization_barrier(jnp.max(decay_map, axis=-1)))
    within = jnp.exp(decay_map - peak[:, :, None])
    across = jnp.exp(carried - peak)
    qfloat = query.astype(jnp.float32)
    products = jnp.einsum('htd,hsd->hts', qfloat, keyrow.astype(jnp.float32))
    scores = products * key_scale * within
    denominator = lax.optimization_barrier(jnp.sum(scores, axis=-1)) + across * jnp.einsum('hd,htd->ht', normer, qfloat, precision=exact)
    weights = scores.astype(jnp.bfloat16)
    numerator = jnp.einsum('hts,hsd->htd', weights.astype(jnp.float32), valrow.astype(jnp.float32))
    numerator = numerator + across[:, :, None] * jnp.einsum('hed,htd->hte', memory, qfloat, precision=exact)
    output = numerator / jnp.maximum(jnp.abs(denominator), jnp.exp(-peak))[:, :, None]
    span_end = cumulative[:, -1]
    gap_log = span_end[:, None] - cumulative + in_gate
    new_peak = jnp.maximum(span_end + stabil, lax.optimization_barrier(jnp.max(gap_log, axis=-1)))
    shrink = jnp.exp(span_end + stabil - new_peak)
    spread = jnp.exp(gap_log - new_peak[:, None]) * key_scale
    keys_weighted = keyrow.astype(jnp.float32) * spread[:, :, None]
    memory = shrink[:, None, None] * memory + jnp.einsum('hse,hsd->hed', valrow.astype(jnp.float32), keys_weighted, precision=exact)
    normer = shrink[:, None] * normer + lax.optimization_barrier(jnp.sum(keys_weighted, axis=1))
    return ((memory, normer, new_peak), output)

def reference(memory_query_matrix, memory_key_matrix, memory_value_matrix, input_gate_logits, forget_gate_logits, forget_log_boosts, head_norm_scale, memory_output_matrix, projection_norm_scale, second_batch_rows, expert_prenorm_scale, selected_expert_index, group_route_probability, expert_choice_scores, expert_gate_matrix, expert_up_matrix, expert_down_matrix):
    spans = SEQ_LEN // SPAN

    def by_head(rows):
        return rows.reshape(SEQ_LEN, HEADS, HEAD_SIZE).transpose(1, 0, 2)

    def to_spans(values):
        shaped = values.reshape((HEADS, spans, SPAN) + values.shape[2:])
        return jnp.moveaxis(shaped, 1, 0)
    log_retain_factor = jax.nn.log_sigmoid(forget_gate_logits) + forget_log_boosts
    start = (jnp.zeros((HEADS, HEAD_SIZE, HEAD_SIZE), jnp.float32), jnp.zeros((HEADS, HEAD_SIZE), jnp.float32), jnp.full((HEADS,), floor_log, jnp.float32))
    inputs = (to_spans(by_head(memory_query_matrix)), to_spans(by_head(memory_key_matrix)), to_spans(by_head(memory_value_matrix)), to_spans(input_gate_logits), to_spans(log_retain_factor))
    _, cells = lax.scan(span_step, start, inputs)
    cells = jnp.moveaxis(cells, 0, 1).reshape(HEADS, SEQ_LEN, HEAD_SIZE)
    scaled = (cells * head_norm_scale.reshape(HEADS, 1, HEAD_SIZE)).astype(jnp.bfloat16)
    head_out = scaled.transpose(1, 0, 2).reshape(SEQ_LEN, CELL_WIDTH)
    projected = jnp.dot(head_out, memory_output_matrix, preferred_element_type=jnp.float32)
    mixed_rows = rms_scale(projected, projection_norm_scale).astype(jnp.bfloat16)
    ffn_rows = rms_scale(second_batch_rows.astype(jnp.float32), expert_prenorm_scale).astype(jnp.bfloat16)
    flat_ids = selected_expert_index.reshape(-1).astype(jnp.int32)
    owners = jnp.repeat(jnp.arange(ROUTED, dtype=jnp.int32), TOPK)
    onehot = (flat_ids[:, None] == jnp.arange(EXPERTS, dtype=jnp.int32)[None, :]).astype(jnp.int32)
    rank = lax.optimization_barrier(jnp.sum((jnp.cumsum(onehot, axis=0) - onehot) * onehot, axis=1)).astype(jnp.int32)
    slots = ROUTED // ROUTED_DEV * CAPACITY
    route_weight = group_route_probability[:, None] * jax.nn.softmax(expert_choice_scores, axis=-1)
    members = jnp.zeros((EXPERTS, slots), jnp.int32).at[flat_ids, rank].set(owners)
    shares = jnp.zeros((EXPERTS, slots), jnp.float32).at[flat_ids, rank].set(route_weight.reshape(-1))

    def one_expert(total, inputs):
        w_gate, w_up, w_down, member_rows, member_shares = inputs
        chosen = ffn_rows[member_rows]
        gate = jnp.dot(chosen, w_gate, preferred_element_type=jnp.float32)
        upper = jnp.dot(chosen, w_up, preferred_element_type=jnp.float32)
        hidden = (jax.nn.silu(gate) * upper).astype(jnp.bfloat16)
        answer = jnp.dot(hidden, w_down, preferred_element_type=jnp.float32).astype(jnp.bfloat16)
        total = total.at[member_rows].add(member_shares[:, None] * answer.astype(jnp.float32))
        return (total, None)
    total, _ = lax.scan(one_expert, jnp.zeros((ROUTED, D), jnp.float32), (expert_gate_matrix, expert_up_matrix, expert_down_matrix, members, shares))
    routed_rows = total.astype(jnp.bfloat16)
    return (mixed_rows, routed_rows)
```

```python
import functools

import jax
import jax.numpy as jnp
from jax import lax
from jax.experimental import pallas as pl
from jax.experimental.pallas import tpu as pltpu
from jax.sharding import Mesh
from jax.sharding import PartitionSpec as P

EP = ("ep_0", "ep_1", "ep_2")
EP_TP = ("ep_0", "ep_1", "ep_2", "tp")
NZ = 8
CAP = 12
HOPS = (4, 3, 3, 2)
SENT = (4, 4, 3, 1)
ORDER = """
S,1,3 S,1,0 summary S,1,2 S,1,1 meta local pick,0 gate,0 give,0,1 give,0,0 S,2,2
S,2,0 S,2,1 pick,1 weigh,0,1 S,2,3 weigh,0,0 S,3,2 gate,1 give,1,1 S,3,1 S,3,0 pick,2
inside pick,3 S,4,0 gate,2 give,2,1 weigh,1,1 gate,3 give,3,1 weigh,2,1 P,2,3,1 give,3,0 pick,4
give,2,0 across P,1,3,1 weigh,3,1 P,3,2,1 P,3,1,1 P,2,2,1 weigh,3,0 P,3,1,0 P,1,2,1 P,3,2,0 gate,4
give,4,1 P,2,1,1 weigh,2,0 P,2,3,0 cells give,4,0 give,1,0 P,2,2,0 weigh,4,1 P,4,0,1 project weigh,4,0
P,2,1,0 P,4,0,0 weigh,1,0 P,1,1,0 P,3,0,0 P,3,0,1 P,2,0,0 P,1,1,1 P,2,0,1 P,1,0,0 P,1,0,1 P,1,3,0
P,1,2,0 final,1 final,0
"""
ROUNDS = (0, 1, 4, 3, 2)

floor_log = -1e30
norm_eps = 1e-06
f32 = jnp.float32
bf16 = jnp.bfloat16
MESH = pl.DeviceIdType.MESH


def iota(shape, dim):
    return lax.broadcasted_iota(jnp.int32, shape, dim)


def dot(a, b):
    return jnp.dot(a, b, preferred_element_type=f32)


def dot_t(a, b):
    return lax.dot_general(a, b, (((0,), (0,)), ((), ())), preferred_element_type=f32)


def dot_nt(a, b):
    return lax.dot_general(a, b, (((1,), (1,)), ((), ())), preferred_element_type=f32)


def stacked(rows, width):
    place = iota((8, width), 0)
    out = jnp.zeros((8, width), f32)
    for k, row in enumerate(rows):
        out = jnp.where(place == k, row, out)
    return out


def joined(early, late):
    total_e, peak_e, memory_e, normer_e = early
    total_l, peak_l, memory_l, normer_l = late
    peak = jnp.maximum(total_l + peak_e, peak_l)
    factor_e = jnp.exp(total_l + peak_e - peak)
    factor_l = jnp.exp(peak_l - peak)
    memory = None if memory_e is None else factor_e * memory_e + factor_l * memory_l
    return (total_e + total_l, peak, memory, factor_e * normer_e + factor_l * normer_l)


def body(
    dims,
    *refs,
):
    given, made, (
        x_ref,
        ids_ref,
        prob_ref,
        score_ref,
        gain_ref,
        q_ref,
        k_ref,
        v_ref,
        ig_ref,
        fg_ref,
        fb_ref,
        hscale_ref,
        pscale_ref,
        wg,
        wu,
        wd,
        wo,
    ), mine = refs[:17], refs[17:19], refs[19:36], refs[36:]
    mixed_hbm, routed_hbm = made
    (
        xn,
        mixed_ref,
        routed_ref,
        hid,
        lead_s,
        into_s,
        xd,
        perm,
        own_meta,
        md,
        mz,
        dz,
        gb,
        rb,
        ob,
        yb,
        ts,
        tr,
        acc,
        ct,
        sm,
        sl,
        sm_all,
        zs_out,
        zm_out,
        zt,
        zm,
        ep_slice,
        ep_meta,
        es,
        ent,
        num_loc,
        lpeak_s,
        den_s,
        bcol_s,
        hs,
        hb,
        w_sem,
        meta_send,
        meta_recv,
        z_send,
        z_recv,
        b_send,
        b_recv,
        x_send,
        x_recv,
        y_send,
        y_recv,
        s_send,
        s_recv,
        t_send,
        t_recv,
        e_send,
        e_recv,
        h_send,
        h_recv,
    ) = mine
    nx, nc, ny = dims
    slab = nx * nc
    tokens, width = x_ref.shape
    part = tokens // 4
    span = q_ref.shape[0]
    size = q_ref.shape[1]
    piece = size // slab
    cols = min(512, width)
    z, xx, cc, yy = (lax.axis_index(a) for a in EP_TP)
    me = xx * nc + cc

    def z_peer(step):
        return (lax.rem(z + step + NZ, NZ), xx, cc, yy)

    def slab_peer(k):
        place = lax.rem(me + k, slab)
        return place, (z, place // nc, lax.rem(place, nc), yy)

    def y_peer(k):
        place = lax.rem(yy + k, ny)
        return place, (z, xx, cc, place)

    pending = []

    def remote(src, dst, send, recv, device):
        return pltpu.make_async_remote_copy(
            src_ref=src, dst_ref=dst, send_sem=send, recv_sem=recv, device_id=device, device_id_type=MESH
        )

    def go(copy):
        copy.start()
        pending.append(copy)

    barrier = pltpu.get_barrier_semaphore()
    greeted = [z_peer(k) for k in range(1, NZ)]
    greeted += [slab_peer(k)[1] for k in range(1, slab)]
    greeted += [y_peer(k)[1] for k in range(1, ny)]
    for device in greeted:
        pl.semaphore_signal(barrier, inc=1, device_id=device, device_id_type=MESH)

    loads = []
    for k, (src, dst) in enumerate(zip(given, refs[19:36])):
        load = pltpu.make_async_copy(src.at[0] if len(src.shape) == 3 else src, dst, w_sem.at[k])
        load.start()
        loads.append(load)
    held = set()

    def need(*numbers):
        for k in numbers:
            if k not in held:
                held.add(k)
                loads[k].wait()

    need(0, 1, 2, 3, 4)

    rows = x_ref[...].astype(f32)
    squares = jnp.mean(rows * rows, axis=-1, keepdims=True)
    xn[...] = (rows * lax.rsqrt(squares + norm_eps) * gain_ref[...]).astype(bf16)

    experts = NZ * slab
    ids = ids_ref[...].astype(f32)
    e0, e1 = ids[0:1, :], ids[1:2, :]
    prob, s0, s1 = prob_ref[...], score_ref[0:1, :], score_ref[1:2, :]
    lanes = iota((experts, tokens), 0).astype(f32)
    oh0, oh1 = (e0 == lanes).astype(f32), (e1 == lanes).astype(f32)
    before = (iota((tokens, tokens), 0) < iota((tokens, tokens), 1)).astype(bf16)
    counts = dot((oh0 + oh1).astype(bf16), before)
    r0 = jnp.sum(counts * oh0, axis=0, keepdims=True)
    r1 = jnp.sum(counts * oh1, axis=0, keepdims=True)
    zf = z.astype(f32)

    def distance(e):
        d = jnp.floor(e * (1.0 / slab)) - zf
        return jnp.where(d < 0, d + NZ, d)

    def either(d):
        return jnp.where((d0 == d) | (d1 == d), 1.0, 0.0)

    d0, d1 = distance(e0), distance(e1)
    opposite = either(4)
    rank = dot(stacked([opposite], tokens).astype(bf16), before)[0:1]
    first = [jnp.where(rank < part, opposite, 0.0), jnp.where(rank < part, 0.0, opposite)]
    classes = []
    for way, far in ((0, 3), (1, 5)):
        second = either(far) * (1.0 - first[way])
        classes += [first[way], second, 1.0 - first[way] - second]
    ranks = dot(stacked(classes, tokens).astype(bf16), before)
    high = jnp.maximum(s0, s1)
    a0, a1 = jnp.exp(s0 - high), jnp.exp(s1 - high)
    w0, w1 = prob * a0 / (a0 + a1), prob * a1 / (a0 + a1)
    own_meta[...] = stacked([e0, r0, e1, r1, w0, w1], tokens)
    slots = iota((tokens, tokens), 0).astype(f32)
    for way in range(2):
        c0, c1, c2 = classes[3 * way : 3 * way + 3]
        n0 = jnp.sum(c0, axis=1, keepdims=True)
        n1 = jnp.sum(c1, axis=1, keepdims=True)
        place = (
            c0 * ranks[3 * way : 3 * way + 1]
            + c1 * (n0 + ranks[3 * way + 1 : 3 * way + 2])
            + c2 * (n0 + n1 + ranks[3 * way + 2 : 3 * way + 3])
        )
        order = (slots == place).astype(bf16)
        perm[way] = order
        other = first[1 - way] > 0.5
        f0 = jnp.where((d0 == 4) & other, 127.0, e0)
        f1 = jnp.where((d1 == 4) & other, 127.0, e1)
        table = stacked([f0, r0, f1, r1, w0, w1], tokens).astype(bf16)
        md[way] = dot_nt(table, order)
        for n in range(0, width, cols):
            xd[way, :, n : n + cols] = dot(order, xn[:, n : n + cols]).astype(bf16)

    pl.semaphore_wait(barrier, len(greeted))

    ways = ((0, 1), (1, -1))

    def chunk(c):
        return pl.ds(c * part, part)

    def outward(h, c, way, step):
        src = xd.at[way, chunk(c)] if h == 1 else dz.at[way, h - 2, chunk(c)]
        return remote(
            src, dz.at[way, h - 1, chunk(c)], z_send.at[way, h - 1, c], z_recv.at[way, h - 1, c], z_peer(step)
        )

    landed = set()

    def arrived(h, c, way, step):
        if (h, c, way) not in landed:
            landed.add((h, c, way))
            outward(h, c, way, step).wait_recv()

    def send(h, c):
        for way, step in ways:
            if h > 1:
                arrived(h - 1, c, way, step)
            go(outward(h, c, way, step))

    def meta_copy(way, step, h):
        return remote(
            md.at[way], mz.at[way, h - 1], meta_send.at[way, h - 1], meta_recv.at[way, h - 1], z_peer(step * h)
        )

    halves = 2
    half = width // halves

    def side(s):
        return pl.ds(s * half, half)

    def homeward(h, c, s, way, step):
        return remote(
            ts.at[way, h - 1, chunk(c), side(s)],
            tr.at[way, h - 1, chunk(c), side(s)],
            b_send.at[way, h - 1, c, s],
            b_recv.at[way, h - 1, c, s],
            z_peer(-step),
        )

    def room(r):
        return 16 if r in (0, 4) else 2 * CAP

    def wanted(r, part_of):
        count = slab * room(r)
        at = iota((count, 1), 0)
        expert = jnp.zeros((count, 1), jnp.int32)
        for k in range(1, slab):
            expert = expert + jnp.where(at >= k * room(r), 1, 0)
        within = at - expert * room(r) - part_of * CAP
        good = (within >= 0) & (within < CAP)
        return jnp.where(good, (z * slab + expert) * CAP + within, -1).astype(f32)

    def streams(r):
        if r == 0:
            return [(own_meta, None, tokens, 0)]
        taken = SENT[r - 1] * part
        return [(mz.at[way, r - 1], way, taken, 0 if r == 4 else way) for way in range(2)]

    def chosen(meta, taken, want, weighted):
        k0 = meta[0:1, 0:taken] * CAP + meta[1:2, 0:taken]
        k1 = meta[2:3, 0:taken] * CAP + meta[3:4, 0:taken]
        if not weighted:
            return ((k0 == want) | (k1 == want)).astype(bf16)
        return (
            jnp.where(k0 == want, meta[4:5, 0:taken], 0.0) + jnp.where(k1 == want, meta[5:6, 0:taken], 0.0)
        ).astype(bf16)

    def x_copy(r, src_place, dst_place, device):
        rows_of = pl.ds(pl.multiple_of(dst_place * room(r), 8), room(r))
        lands = pl.ds(pl.multiple_of(src_place * room(r), 8), room(r))
        n = ROUNDS.index(r)
        return remote(
            gb.at[n, rows_of], rb.at[n, lands], x_send.at[n, dst_place], x_recv.at[n, src_place], device
        )

    def y_copy(r, s, src_place, dst_place, device):
        rows_of = pl.ds(pl.multiple_of(dst_place * room(r), 8), room(r))
        lands = pl.ds(pl.multiple_of(src_place * room(r), 8), room(r))
        n = ROUNDS.index(r)
        return remote(
            ob.at[n, rows_of, side(s)],
            yb.at[n, lands, side(s)],
            y_send.at[n, dst_place, s],
            y_recv.at[n, src_place, s],
            device,
        )

    def pick(r):
        n, count = ROUNDS.index(r), slab * room(r)
        if r:
            known(r)
        for c in range(SENT[r - 1] if r else 0):
            for way, step in ways:
                arrived(r, c, way, step)
        picks = []
        for meta, way, taken, second in streams(r):
            picks.append((chosen(meta[...], taken, wanted(r, second), False), way, taken))

        @pl.loop(0, width // cols)
        def _(t):
            at = pl.ds(pl.multiple_of(t * cols, 128), cols)
            total = jnp.zeros((count, cols), f32)
            for one_hot, way, taken in picks:
                source = xn[0:taken, at] if way is None else dz[way, r - 1, 0:taken, at]
                total = total + dot(one_hot, source)
            gb[n, 0:count, at] = total.astype(bf16)

        for k in range(1, slab):
            place, device = slab_peer(k)
            go(x_copy(r, me, place, device))
        own = pl.ds(pl.multiple_of(me * room(r), 8), room(r))
        rb[n, own, :] = gb[n, own, :]

    def gate(r):
        n, count = ROUNDS.index(r), slab * room(r)
        for k in range(1, slab):
            place, device = slab_peer(k)
            x_copy(r, place, me, device).wait_recv()
        need(13, 14)
        rows = rb[n, 0:count, :]
        value = dot(rows, wg[...])
        hid[n, 0:count, :] = (value / (1.0 + jnp.exp(-value)) * dot(rows, wu[...])).astype(bf16)

    def give(r, s):
        n, count = ROUNDS.index(r), slab * room(r)
        need(15)
        hidden = hid[n, 0:count, :]

        @pl.loop(0, half // cols)
        def _(t):
            at = pl.ds(pl.multiple_of(s * half + t * cols, 128), cols)
            ob[n, 0:count, at] = dot(hidden, wd[:, at]).astype(bf16)

        for k in range(1, slab):
            place, device = slab_peer(k)
            go(y_copy(r, s, me, place, device))
        own = pl.ds(pl.multiple_of(me * room(r), 8), room(r))
        yb[n, own, side(s)] = ob[n, own, side(s)]

    def weigh(r, s):
        n, count = ROUNDS.index(r), slab * room(r)
        for k in range(1, slab):
            place, device = slab_peer(k)
            y_copy(r, s, place, me, device).wait_recv()
        parts = []
        for meta, way, taken, second in streams(r):
            parts.append((chosen(meta[...], taken, wanted(r, second), True), way, taken))

        @pl.loop(0, half // cols)
        def _(t):
            at = pl.ds(pl.multiple_of(s * half + t * cols, 128), cols)
            for weights, way, taken in parts:
                value = dot_t(weights, yb[n, 0:count, at])
                if way is None:
                    acc[:, at] = value
                else:
                    ts[way, r - 1, 0:taken, at] = value.astype(bf16)

    def pass_on(h, c, s):
        for way, step in ways:
            if h < 4 and c < SENT[h]:
                homeward(h + 1, c, s, way, step).wait_recv()
                at = slice(c * part, (c + 1) * part)
                ts[way, h - 1, at, side(s)] = (
                    ts[way, h - 1, at, side(s)].astype(f32) + tr[way, h, at, side(s)].astype(f32)
                ).astype(bf16)
            go(homeward(h, c, s, way, step))

    def finish(s):
        for c in range(4):
            for way, step in ways:
                homeward(1, c, s, way, step).wait_recv()

        @pl.loop(0, half // cols)
        def _(t):
            at = pl.ds(pl.multiple_of(s * half + t * cols, 128), cols)
            total = acc[:, at]
            for way in range(2):
                total = total + dot_t(perm[way], tr[way, 0, :, at])
            routed_ref[:, at] = total.astype(bf16)

        out = pltpu.make_async_copy(routed_ref.at[:, side(s)], routed_hbm.at[:, side(s)], w_sem.at[17 + s])
        out.start()
        leaving.append(out)

    leaving = []

    key_scale = size**-0.5

    def summary():
        need(6, 7, 8, 9, 10)
        gate = fg_ref[...]
        keep = jnp.minimum(gate, 0.0) - jnp.log1p(jnp.exp(-jnp.abs(gate))) + fb_ref[...]
        upto = (iota((span, span), 0) <= iota((span, span), 1)).astype(f32)
        total = jnp.dot(
            stacked([keep], span), upto, preferred_element_type=f32, precision=lax.Precision.HIGHEST
        )[0:1]
        lead = ig_ref[...] - total
        last = total[:, span - 1 : span]
        top = jnp.max(last + lead, axis=1, keepdims=True)
        spread = jnp.exp(last + lead - top) * key_scale
        unit = (iota((8, 8), 0) == iota((8, 8), 1)).astype(f32)
        columns = lax.dot_general(
            stacked([total, spread], span),
            unit,
            (((0,), (0,)), ((), ())),
            preferred_element_type=f32,
            precision=lax.Precision.HIGHEST,
        )
        bcol_s[...] = columns[:, 0:1]
        weighted = k_ref[...].astype(f32) * columns[:, 1:2]
        ct[...] = dot_t(weighted.astype(bf16), v_ref[...])
        normer = jnp.sum(weighted, axis=0, keepdims=True)
        wide = jnp.zeros((1, size), f32)
        sm[...] = stacked([normer, last + wide, top + wide], size)
        for k in range(1, slab):
            place, device = slab_peer(k)
            for copy in s_copies(me, place, device):
                go(copy)
        sl[me] = ct[pl.ds(pl.multiple_of(me * piece, 8), piece), :]
        sm_all[me] = sm[...]
        lead_s[...] = lead

    def s_copies(src_place, dst_place, device):
        return (
            remote(
                ct.at[pl.ds(pl.multiple_of(dst_place * piece, 8), piece)],
                sl.at[src_place],
                s_send.at[0, dst_place],
                s_recv.at[0, src_place],
                device,
            ),
            remote(sm, sm_all.at[src_place], s_send.at[1, dst_place], s_recv.at[1, src_place], device),
        )

    def local():
        need(5)
        lead = lead_s[...]
        block = min(128, span)
        for at in range(0, span, block):
            end = at + block
            q = q_ref[at:end, :]
            products = dot_nt(q, k_ref[0:end, :]) * key_scale
            decay = bcol_s[at:end, :] + lead[:, 0:end]
            decay = jnp.where(iota((block, end), 1) <= iota((block, end), 0) + at, decay, floor_log)
            peak = jnp.max(decay, axis=1, keepdims=True)
            scores = products * jnp.exp(decay - peak)
            lpeak_s[at:end, :] = peak
            den_s[at:end, :] = jnp.sum(scores, axis=1, keepdims=True)
            num_loc[at:end, :] = dot(scores.astype(bf16), v_ref[0:end, :])

    def t_copies(src_z, k):
        return (
            remote(zs_out, zt.at[src_z], t_send.at[0, k], t_recv.at[0, src_z], z_peer(k)),
            remote(zm_out, zm.at[src_z], t_send.at[1, k], t_recv.at[1, src_z], z_peer(k)),
        )

    def unpacked(meta, memory):
        return (meta[1:2, :], meta[2:3, :], memory, meta[0:1, :])

    def nothing():
        zero = jnp.zeros((1, size), f32)
        return (zero, zero + floor_log, jnp.zeros((piece, size), f32), zero)

    def inside():
        for k in range(1, slab):
            place, device = slab_peer(k)
            for copy in s_copies(place, me, device):
                copy.wait_recv()
        state = nothing()
        for p in range(slab):
            ep_slice[p] = state[2]
            ep_meta[p] = stacked([state[3], state[0], state[1]], size)
            state = joined(state, unpacked(sm_all[p], sl[p]))
        zs_out[...] = state[2].astype(bf16)
        zm_out[...] = stacked([state[3], state[0], state[1]], size)
        for k in range(1, NZ):
            for copy in t_copies(z, k):
                go(copy)

    def e_copy(src_place, dst_place, device):
        return remote(
            es.at[dst_place],
            ent.at[pl.ds(pl.multiple_of(src_place * piece, 16), piece)],
            e_send.at[dst_place],
            e_recv.at[src_place],
            device,
        )

    def across():
        for k in range(1, NZ):
            for copy in t_copies(lax.rem(z + k, NZ), NZ - k):
                copy.wait_recv()
        zt[z] = zs_out[...]
        zm[z] = zm_out[...]
        state = nothing()
        for s in range(NZ - 1):
            earlier = s < z
            total, peak, memory, normer = unpacked(zm[s], zt[s].astype(f32))
            part_of = (
                jnp.where(earlier, total, 0.0),
                jnp.where(earlier, peak, floor_log),
                jnp.where(earlier, memory, 0.0),
                jnp.where(earlier, normer, 0.0),
            )
            state = joined(state, part_of)
        for p in range(slab):
            es[p] = joined(state, unpacked(ep_meta[p], ep_slice[p]))[2].astype(bf16)
        for k in range(1, slab):
            place, device = slab_peer(k)
            go(e_copy(me, place, device))
        ent[pl.ds(pl.multiple_of(me * piece, 16), piece), :] = es[me]
        total, peak, _, normer = state
        both = joined((total, peak, None, normer), unpacked(ep_meta[me], None))
        into_s[...] = stacked([both[3], both[0], both[1]], size)

    def h_copy(src_y, dst_y, device):
        quarter = span // ny
        return remote(
            hs.at[pl.ds(pl.multiple_of(dst_y * quarter, 16), quarter)],
            hb.at[src_y],
            h_send.at[dst_y],
            h_recv.at[src_y],
            device,
        )

    def cells():
        need(11)
        _, stabil, _, normer = unpacked(into_s[...], None)
        for k in range(1, slab):
            place, device = slab_peer(k)
            e_copy(place, me, device).wait_recv()
        block = min(256, span)
        for at in range(0, span, block):
            end = at + block
            q = q_ref[at:end, :]
            carried = bcol_s[at:end, :] + stabil[:, 0:1]
            peak = jnp.maximum(carried, lpeak_s[at:end, :])
            factor = jnp.exp(lpeak_s[at:end, :] - peak)
            across_ = jnp.exp(carried - peak)
            den = factor * den_s[at:end, :] + across_ * jnp.sum(q.astype(f32) * normer, axis=1, keepdims=True)
            num = factor * num_loc[at:end, :] + across_ * dot(q, ent[...])
            cell = num / jnp.maximum(jnp.abs(den), jnp.exp(-peak))
            hs[at:end, :] = (cell * hscale_ref[...]).astype(bf16)
        quarter = span // ny
        for k in range(1, ny):
            place, device = y_peer(k)
            go(h_copy(yy, place, device))
        hb[yy] = hs[pl.ds(pl.multiple_of(yy * quarter, 16), quarter), :]

    def project():
        for k in range(1, ny):
            place, device = y_peer(k)
            h_copy(place, yy, device).wait_recv()
        need(12, 16)
        quarter = span // ny
        total = jnp.zeros((quarter, width), f32)
        for y in range(ny):
            total = total + dot(hb[y], wo[y * size : (y + 1) * size, :])
        squares = jnp.mean(total * total, axis=-1, keepdims=True)
        mixed_ref[...] = (total * lax.rsqrt(squares + norm_eps) * pscale_ref[...]).astype(bf16)
        out = pltpu.make_async_copy(mixed_ref, mixed_hbm, w_sem.at[19])
        out.start()
        leaving.append(out)

    def tables():
        for way, step in ways:
            for h in range(1, 5):
                go(meta_copy(way, step, h))

    told = set()

    def known(h):
        if h not in told:
            told.add(h)
            for way, step in ways:
                meta_copy(way, step, h).wait_recv()

    steps = dict(
        S=send,
        meta=tables,
        pick=pick,
        gate=gate,
        give=give,
        weigh=weigh,
        P=pass_on,
        summary=summary,
        local=local,
        inside=inside,
        across=across,
        cells=cells,
        project=project,
        final=finish,
    )
    for line in ORDER.split():
        name, *numbers = line.split(",")
        steps[name](*(int(k) for k in numbers))
    for copy in pending:
        copy.wait_send()
    for copy in leaving:
        copy.wait()


def copied(a_ref, b_ref, a_out, b_out, a_held, b_held, sems):
    moves = []
    for n, (src, held, dst) in enumerate(((a_ref, a_held, a_out), (b_ref, b_held, b_out))):
        block = src.shape[0] // 2
        for k in range(2):
            at = pl.ds(k * block, block)
            into = pltpu.make_async_copy(src.at[at], held.at[at], sems.at[n, k, 0])
            into.start()
            moves.append((into, pltpu.make_async_copy(held.at[at], dst.at[at], sems.at[n, k, 1])))
    for into, out in moves:
        into.wait()
        out.start()
    for _, out in moves:
        out.wait()


def shards(
    memory_query_matrix,
    memory_key_matrix,
    memory_value_matrix,
    input_gate_logits,
    forget_gate_logits,
    forget_log_boosts,
    head_norm_scale,
    memory_output_matrix,
    projection_norm_scale,
    second_batch_rows,
    expert_prenorm_scale,
    selected_expert_index,
    group_route_probability,
    expert_choice_scores,
    expert_gate_matrix,
    expert_up_matrix,
    expert_down_matrix,
):
    nx, nc, ny = (lax.axis_size(a) for a in ("ep_1", "ep_2", "tp"))
    slab = nx * nc
    tokens, width = second_batch_rows.shape
    span, size = memory_query_matrix.shape
    hidden = expert_gate_matrix.shape[2]
    piece = size // slab
    part = tokens // 4
    cellw = memory_output_matrix.shape[0]
    most = slab * 2 * CAP
    anywhere = pl.BlockSpec(memory_space=pl.ANY)
    dma = pltpu.SemaphoreType.DMA
    rounds = len(ROUNDS)
    inputs = (
        second_batch_rows,
        selected_expert_index.T,
        group_route_probability[None, :],
        expert_choice_scores.T,
        expert_prenorm_scale[None, :],
        memory_query_matrix,
        memory_key_matrix,
        memory_value_matrix,
        input_gate_logits,
        forget_gate_logits,
        forget_log_boosts,
        head_norm_scale[None, :],
        projection_norm_scale[None, :],
        expert_gate_matrix,
        expert_up_matrix,
        expert_down_matrix,
        memory_output_matrix,
    )
    scratch = [pltpu.VMEM(a.shape[-2:], a.dtype) for a in inputs]
    scratch += [
        pltpu.VMEM((tokens, width), bf16),
        pltpu.VMEM((span // ny, width), bf16),
        pltpu.VMEM((tokens, width), bf16),
        pltpu.VMEM((rounds, most, hidden), bf16),
        pltpu.VMEM((1, span), f32),
        pltpu.VMEM((8, size), f32),
        pltpu.VMEM((2, tokens, width), bf16),
        pltpu.VMEM((2, tokens, tokens), bf16),
        pltpu.VMEM((8, tokens), f32),
        pltpu.VMEM((2, 8, tokens), f32),
        pltpu.VMEM((2, 4, 8, tokens), f32),
        pltpu.VMEM((2, 4, tokens, width), bf16),
        pltpu.VMEM((rounds, most, width), bf16),
        pltpu.VMEM((rounds, most, width), bf16),
        pltpu.VMEM((rounds, most, width), bf16),
        pltpu.VMEM((rounds, most, width), bf16),
        pltpu.VMEM((2, 4, tokens, width), bf16),
        pltpu.VMEM((2, 4, tokens, width), bf16),
        pltpu.VMEM((tokens, width), f32),
        pltpu.VMEM((size, size), f32),
        pltpu.VMEM((8, size), f32),
        pltpu.VMEM((slab, piece, size), f32),
        pltpu.VMEM((slab, 8, size), f32),
        pltpu.VMEM((piece, size), bf16),
        pltpu.VMEM((8, size), f32),
        pltpu.VMEM((NZ, piece, size), bf16),
        pltpu.VMEM((NZ, 8, size), f32),
        pltpu.VMEM((slab, piece, size), f32),
        pltpu.VMEM((slab, 8, size), f32),
        pltpu.VMEM((slab, piece, size), bf16),
        pltpu.VMEM((size, size), bf16),
        pltpu.VMEM((span, size), f32),
        pltpu.VMEM((span, 1), f32),
        pltpu.VMEM((span, 1), f32),
        pltpu.VMEM((span, 1), f32),
        pltpu.VMEM((span, size), bf16),
        pltpu.VMEM((ny, span // ny, size), bf16),
        dma((20,)),
        dma((2, 4)),
        dma((2, 4)),
        dma((2, 4, 4)),
        dma((2, 4, 4)),
        dma((2, 4, 4, 2)),
        dma((2, 4, 4, 2)),
        dma((rounds, slab)),
        dma((rounds, slab)),
        dma((rounds, slab, 2)),
        dma((rounds, slab, 2)),
        dma((2, slab)),
        dma((2, slab)),
        dma((2, NZ)),
        dma((2, NZ)),
        dma((slab,)),
        dma((slab,)),
        dma((ny,)),
        dma((ny,)),
    ]
    shapes = (
        jax.ShapeDtypeStruct((span // ny, width), bf16),
        jax.ShapeDtypeStruct((tokens, width), bf16),
    )
    mixed, routed = pl.pallas_call(
        functools.partial(body, (nx, nc, ny)),
        out_shape=shapes,
        in_specs=[anywhere] * len(inputs),
        out_specs=(anywhere, anywhere),
        scratch_shapes=scratch,
        compiler_params=pltpu.CompilerParams(
            collective_id=0, has_side_effects=True, vmem_limit_bytes=67043328
        ),
    )(*inputs)
    return pl.pallas_call(
        copied,
        out_shape=shapes,
        in_specs=[anywhere] * 2,
        out_specs=(anywhere, anywhere),
        scratch_shapes=[
            pltpu.VMEM(shapes[0].shape, bf16),
            pltpu.VMEM(shapes[1].shape, bf16),
            dma((2, 2, 2)),
        ],
    )(mixed, routed)


def solution(mesh):
    finer = Mesh(mesh.devices.reshape(8, 4, 2, mesh.shape["tp"]), EP_TP)
    in_specs = (
        P(EP, "tp"),
        P(EP, "tp"),
        P(EP, "tp"),
        P("tp", EP),
        P("tp", EP),
        P("tp", EP),
        P("tp"),
        P(),
        P(),
        P(EP_TP, None),
        P(),
        P(EP_TP, None),
        P(EP_TP),
        P(EP_TP, None),
        P(EP, None, None),
        P(EP, None, None),
        P(EP, None, None),
    )
    out_specs = (P(EP_TP, None), P(EP_TP, None))
    return jax.shard_map(shards, mesh=finer, in_specs=in_specs, out_specs=out_specs, check_vma=False)
```

```python
import functools

import jax
import jax.numpy as jnp
from jax import lax
from jax.experimental import pallas as pl
from jax.experimental.pallas import tpu as pltpu
from jax.sharding import Mesh
from jax.sharding import PartitionSpec as P

EP = ("ep_0", "ep_1", "ep_2")
EP_TP = ("ep_0", "ep_1", "ep_2", "tp")
NZ = 8
CAP = 12
HOPS = (4, 3, 3, 2)
SENT = (4, 4, 3, 1)
ORDER = """
S,1,0,1 S,1,1,0 S,1,3,0 S,1,0,0 S,1,2,0 pick,0,1 pick,0,0 S,1,1,1 S,1,3,1 gate,0 pick,1,0 S,1,2,1
S,2,2,0 S,2,3,0 S,2,1,0 S,2,0,0 summary pick,1,1 S,2,2,1 S,2,3,1 S,2,1,1 S,2,0,1 local S,3,0,0
pick,2,0 gate,1 give,1,1 S,3,2,0 pick,2,1 S,3,1,0 S,3,0,1 S,3,2,1 pick,3,0 S,3,1,1 S,4,0,0 weigh,1,1
gate,2 give,2,1 pick,3,1 give,2,0 weigh,2,1 inside P,2,3,1 S,4,0,1 gate,3 give,3,1 give,3,0 P,1,3,1
far pick,4,1 weigh,2,0 P,2,3,0 weigh,3,1 P,3,1,1 P,3,2,1 pick,4,0 P,2,1,1 weigh,3,0 P,3,1,0 give,1,0
P,3,2,0 P,2,2,1 gate,4 give,4,0 P,2,1,0 across P,1,1,1 weigh,1,0 give,4,1 P,1,2,1 give,0,1 P,1,3,0
P,2,2,0 weigh,4,1 give,0,0 weigh,4,0 P,4,0,0 P,4,0,1 cells P,1,1,0 P,3,0,0 project P,3,0,1 P,2,0,0
P,2,0,1 P,1,0,0 weigh,0,1 P,1,2,0 weigh,0,0 P,1,0,1 final,0 final,1
"""
HALVES = 2
ROUNDS = (0, 1, 4, 3, 2)

floor_log = -1e30
norm_eps = 1e-06
f32 = jnp.float32
bf16 = jnp.bfloat16
MESH = pl.DeviceIdType.MESH


def iota(shape, dim):
    return lax.broadcasted_iota(jnp.int32, shape, dim)


def dot(a, b):
    return jnp.dot(a, b, preferred_element_type=f32)


def dot_t(a, b):
    return lax.dot_general(a, b, (((0,), (0,)), ((), ())), preferred_element_type=f32)


def dot_nt(a, b):
    return lax.dot_general(a, b, (((1,), (1,)), ((), ())), preferred_element_type=f32)


def stacked(rows, width, count=8):
    place = iota((count, width), 0)
    out = jnp.zeros((count, width), f32)
    for k, row in enumerate(rows):
        out = jnp.where(place == k, row, out)
    return out


def joined(early, late):
    total_e, peak_e, memory_e, normer_e = early
    total_l, peak_l, memory_l, normer_l = late
    peak = jnp.maximum(total_l + peak_e, peak_l)
    factor_e = jnp.exp(total_l + peak_e - peak)
    factor_l = jnp.exp(peak_l - peak)
    memory = None if memory_e is None else factor_e * memory_e + factor_l * memory_l
    return (total_e + total_l, peak, memory, factor_e * normer_e + factor_l * normer_l)


def body(
    dims,
    *refs,
):
    given, made, (
        x_ref,
        ids_ref,
        prob_ref,
        score_ref,
        gain_ref,
        q_ref,
        k_ref,
        v_ref,
        ig_ref,
        fg_ref,
        fb_ref,
        hscale_ref,
        pscale_ref,
        wg,
        wu,
        wd,
        wo,
    ), mine = refs[:17], refs[17:19], refs[19:36], refs[36:]
    mixed_hbm, routed_hbm = made
    (
        xn,
        mixed_ref,
        routed_ref,
        hid,
        lead_s,
        into_s,
        xd,
        perm,
        own_meta,
        md,
        mz,
        dz,
        gb,
        rb,
        ob,
        yb,
        ts,
        tr,
        acc,
        ct,
        sm,
        sl,
        sm_all,
        zs_out,
        zm_out,
        zt,
        zm,
        ep_slice,
        ep_meta,
        es,
        ent,
        num_loc,
        lpeak_s,
        den_s,
        bcol_s,
        hs,
        hb,
        w_sem,
        meta_send,
        meta_recv,
        z_send,
        z_recv,
        b_send,
        b_recv,
        x_send,
        x_recv,
        y_send,
        y_recv,
        s_send,
        s_recv,
        t_send,
        t_recv,
        e_send,
        e_recv,
        h_send,
        h_recv,
    ) = mine
    nx, nc, ny = dims
    slab = nx * nc
    tokens, width = x_ref.shape
    part = tokens // 4
    span = q_ref.shape[0]
    size = q_ref.shape[1]
    piece = size // slab
    cols = min(512, width // HALVES)
    z, xx, cc, yy = (lax.axis_index(a) for a in EP_TP)
    me = xx * nc + cc

    def z_peer(step):
        return (lax.rem(z + step + NZ, NZ), xx, cc, yy)

    def slab_peer(k):
        place = lax.rem(me + k, slab)
        return place, (z, place // nc, lax.rem(place, nc), yy)

    def y_peer(k):
        place = lax.rem(yy + k, ny)
        return place, (z, xx, cc, place)

    pending = []

    def remote(src, dst, send, recv, device):
        return pltpu.make_async_remote_copy(
            src_ref=src, dst_ref=dst, send_sem=send, recv_sem=recv, device_id=device, device_id_type=MESH
        )

    def go(copy):
        copy.start()
        pending.append(copy)

    barrier = pltpu.get_barrier_semaphore()
    greeted = [z_peer(1), z_peer(-1)]
    greeted += [slab_peer(k)[1] for k in range(1, slab)]
    greeted += [y_peer(k)[1] for k in range(1, ny)]
    for device in greeted:
        pl.semaphore_signal(barrier, inc=1, device_id=device, device_id_type=MESH)

    loads = []
    for k, (src, dst) in enumerate(zip(given, refs[19:36])):
        load = pltpu.make_async_copy(src.at[0] if len(src.shape) == 3 else src, dst, w_sem.at[k])
        load.start()
        loads.append(load)
    held = set()

    def need(*numbers):
        for k in numbers:
            if k not in held:
                held.add(k)
                loads[k].wait()

    need(0, 1, 2, 3, 4)

    rows = x_ref[...].astype(f32)
    squares = jnp.mean(rows * rows, axis=-1, keepdims=True)
    xn[...] = (rows * lax.rsqrt(squares + norm_eps) * gain_ref[...]).astype(bf16)

    experts = NZ * slab
    ids = ids_ref[...].astype(f32)
    e0, e1 = ids[0:1, :], ids[1:2, :]
    prob, s0, s1 = prob_ref[...], score_ref[0:1, :], score_ref[1:2, :]
    lanes = iota((experts, tokens), 0).astype(f32)
    oh0, oh1 = (e0 == lanes).astype(f32), (e1 == lanes).astype(f32)
    before = (iota((tokens, tokens), 0) < iota((tokens, tokens), 1)).astype(bf16)
    counts = dot((oh0 + oh1).astype(bf16), before)
    r0 = jnp.sum(counts * oh0, axis=0, keepdims=True)
    r1 = jnp.sum(counts * oh1, axis=0, keepdims=True)
    zf = z.astype(f32)

    def distance(e):
        d = jnp.floor(e * (1.0 / slab)) - zf
        return jnp.where(d < 0, d + NZ, d)

    def either(d):
        return jnp.where((d0 == d) | (d1 == d), 1.0, 0.0)

    d0, d1 = distance(e0), distance(e1)
    opposite = either(4)
    rank = dot(stacked([opposite], tokens).astype(bf16), before)[0:1]
    first = [jnp.where(rank < part, opposite, 0.0), jnp.where(rank < part, 0.0, opposite)]
    classes = []
    for way, far in ((0, 3), (1, 5)):
        second = either(far) * (1.0 - first[way])
        classes += [first[way], second, 1.0 - first[way] - second]
    ranks = dot(stacked(classes, tokens).astype(bf16), before)
    high = jnp.maximum(s0, s1)
    a0, a1 = jnp.exp(s0 - high), jnp.exp(s1 - high)
    w0, w1 = prob * a0 / (a0 + a1), prob * a1 / (a0 + a1)
    own_meta[...] = stacked([e0, r0, e1, r1, w0, w1], tokens)
    slots = iota((tokens, tokens), 0).astype(f32)
    for way in range(2):
        c0, c1, c2 = classes[3 * way : 3 * way + 3]
        n0 = jnp.sum(c0, axis=1, keepdims=True)
        n1 = jnp.sum(c1, axis=1, keepdims=True)
        place = (
            c0 * ranks[3 * way : 3 * way + 1]
            + c1 * (n0 + ranks[3 * way + 1 : 3 * way + 2])
            + c2 * (n0 + n1 + ranks[3 * way + 2 : 3 * way + 3])
        )
        order = (slots == place).astype(bf16)
        perm[way] = order
        other = first[1 - way] > 0.5
        f0 = jnp.where((d0 == 4) & other, 127.0, e0)
        f1 = jnp.where((d1 == 4) & other, 127.0, e1)
        table = stacked([f0, r0, f1, r1, w0, w1], tokens).astype(bf16)
        md[way] = dot_nt(table, order).astype(bf16)
        for n in range(0, width, cols):
            xd[way, :, n : n + cols] = dot(order, xn[:, n : n + cols]).astype(bf16)

    pl.semaphore_wait(barrier, len(greeted))

    ways = ((0, 1), (1, -1))

    def chunk(c):
        return pl.ds(c * part, part)

    there = width // 2

    def wing(d):
        return pl.ds(d * there, there)

    def outward(h, c, d, way, step):
        src = xd.at[way, chunk(c), wing(d)] if h == 1 else dz.at[way, h - 2, chunk(c), wing(d)]
        return remote(
            src,
            dz.at[way, h - 1, chunk(c), wing(d)],
            z_send.at[way, h - 1, c, d],
            z_recv.at[way, h - 1, c, d],
            z_peer(step),
        )

    landed = set()
    spread = set()

    def arrived(h, c, d, way, step):
        if (h, c, d, way) not in landed:
            landed.add((h, c, d, way))
            outward(h, c, d, way, step).wait_recv()

    def send(h, c, d):
        for way, step in ways:
            if h > 1:
                arrived(h - 1, c, d, way, step)
            go(outward(h, c, d, way, step))
        if h not in spread:
            spread.add(h)
            known(h - 1)
            for way, step in ways:
                go(meta_copy(way, step, h))

    def meta_copy(way, step, h):
        some = pl.ds(0, tokens if h < 4 else min(tokens, 128))
        src = md.at[way, :, some] if h == 1 else mz.at[way, h - 2, :, some]
        return remote(
            src, mz.at[way, h - 1, :, some], meta_send.at[way, h - 1], meta_recv.at[way, h - 1], z_peer(step)
        )

    told = {}

    def known(h):
        if h and not told.setdefault(h, False):
            told[h] = True
            for way, step in ways:
                meta_copy(way, step, h).wait_recv()

    half = width // HALVES

    def side(s):
        return pl.ds(s * half, half)

    def homeward(h, c, s, way, step):
        return remote(
            ts.at[way, h - 1, chunk(c), side(s)],
            tr.at[way, h - 1, chunk(c), side(s)],
            b_send.at[way, h - 1, c, s],
            b_recv.at[way, h - 1, c, s],
            z_peer(-step),
        )

    def room(r):
        return 16 if r in (0, 4) else 2 * CAP

    def wanted(r, part_of):
        count = slab * room(r)
        at = iota((count, 1), 0)
        expert = jnp.zeros((count, 1), jnp.int32)
        for k in range(1, slab):
            expert = expert + jnp.where(at >= k * room(r), 1, 0)
        within = at - expert * room(r) - part_of * CAP
        good = (within >= 0) & (within < CAP)
        return jnp.where(good, (z * slab + expert) * CAP + within, -1).astype(f32)

    def streams(r):
        if r == 0:
            return [(own_meta, None, tokens, 0)]
        taken = SENT[r - 1] * part
        return [(mz.at[way, r - 1], way, taken, 0 if r == 4 else way) for way in range(2)]

    def chosen(meta, taken, want, weighted):
        k0 = meta[0:1, 0:taken] * CAP + meta[1:2, 0:taken]
        k1 = meta[2:3, 0:taken] * CAP + meta[3:4, 0:taken]
        if not weighted:
            return ((k0 == want) | (k1 == want)).astype(bf16)
        return (
            jnp.where(k0 == want, meta[4:5, 0:taken], 0.0) + jnp.where(k1 == want, meta[5:6, 0:taken], 0.0)
        ).astype(bf16)

    def x_copy(r, d, src_place, dst_place, device):
        rows_of = pl.ds(pl.multiple_of(dst_place * room(r), 8), room(r))
        lands = pl.ds(pl.multiple_of(src_place * room(r), 8), room(r))
        n = ROUNDS.index(r)
        return remote(
            gb.at[n, rows_of, wing(d)],
            rb.at[n, lands, wing(d)],
            x_send.at[n, dst_place, d],
            x_recv.at[n, src_place, d],
            device,
        )

    def y_copy(r, s, src_place, dst_place, device):
        rows_of = pl.ds(pl.multiple_of(dst_place * room(r), 8), room(r))
        lands = pl.ds(pl.multiple_of(src_place * room(r), 8), room(r))
        n = ROUNDS.index(r)
        return remote(
            ob.at[n, rows_of, side(s)],
            yb.at[n, lands, side(s)],
            y_send.at[n, dst_place, s],
            y_recv.at[n, src_place, s],
            device,
        )

    def pick(r, d):
        n, count = ROUNDS.index(r), slab * room(r)
        known(r)
        for c in range(SENT[r - 1] if r else 0):
            for way, step in ways:
                arrived(r, c, d, way, step)
        picks = []
        for meta, way, taken, second in streams(r):
            picks.append((chosen(meta[...].astype(f32), taken, wanted(r, second), False), way, taken))

        @pl.loop(0, there // cols)
        def _(t):
            at = pl.ds(pl.multiple_of(d * there + t * cols, 128), cols)
            total = jnp.zeros((count, cols), f32)
            for one_hot, way, taken in picks:
                source = xn[0:taken, at] if way is None else dz[way, r - 1, 0:taken, at]
                total = total + dot(one_hot, source)
            gb[n, 0:count, at] = total.astype(bf16)

        for k in range(1, slab):
            place, device = slab_peer(k)
            go(x_copy(r, d, me, place, device))
        own = pl.ds(pl.multiple_of(me * room(r), 8), room(r))
        rb[n, own, wing(d)] = gb[n, own, wing(d)]

    def gate(r):
        n, count = ROUNDS.index(r), slab * room(r)
        for k in range(1, slab):
            place, device = slab_peer(k)
            for d in range(2):
                x_copy(r, d, place, me, device).wait_recv()
        need(13, 14)
        rows = rb[n, 0:count, :]
        value = dot(rows, wg[...])
        hid[n, 0:count, :] = (value / (1.0 + jnp.exp(-value)) * dot(rows, wu[...])).astype(bf16)

    def give(r, s):
        n, count = ROUNDS.index(r), slab * room(r)
        need(15)
        hidden = hid[n, 0:count, :]

        @pl.loop(0, half // cols)
        def _(t):
            at = pl.ds(pl.multiple_of(s * half + t * cols, 128), cols)
            ob[n, 0:count, at] = dot(hidden, wd[:, at]).astype(bf16)

        for k in range(1, slab):
            place, device = slab_peer(k)
            go(y_copy(r, s, me, place, device))
        own = pl.ds(pl.multiple_of(me * room(r), 8), room(r))
        yb[n, own, side(s)] = ob[n, own, side(s)]

    def weigh(r, s):
        n, count = ROUNDS.index(r), slab * room(r)
        for k in range(1, slab):
            place, device = slab_peer(k)
            y_copy(r, s, place, me, device).wait_recv()
        parts = []
        for meta, way, taken, second in streams(r):
            parts.append((chosen(meta[...].astype(f32), taken, wanted(r, second), True), way, taken))

        @pl.loop(0, half // cols)
        def _(t):
            at = pl.ds(pl.multiple_of(s * half + t * cols, 128), cols)
            for weights, way, taken in parts:
                value = dot_t(weights, yb[n, 0:count, at])
                if way is None:
                    acc[:, at] = value
                else:
                    ts[way, r - 1, 0:taken, at] = value.astype(bf16)

    def pass_on(h, c, s):
        for way, step in ways:
            if h < 4 and c < SENT[h]:
                homeward(h + 1, c, s, way, step).wait_recv()
                at = slice(c * part, (c + 1) * part)
                ts[way, h - 1, at, side(s)] = (
                    ts[way, h - 1, at, side(s)].astype(f32) + tr[way, h, at, side(s)].astype(f32)
                ).astype(bf16)
            go(homeward(h, c, s, way, step))

    def finish(s):
        for c in range(4):
            for way, step in ways:
                homeward(1, c, s, way, step).wait_recv()

        @pl.loop(0, half // cols)
        def _(t):
            at = pl.ds(pl.multiple_of(s * half + t * cols, 128), cols)
            total = acc[:, at]
            for way in range(2):
                total = total + dot_t(perm[way], tr[way, 0, :, at])
            routed_ref[:, at] = total.astype(bf16)

        out = pltpu.make_async_copy(routed_ref.at[:, side(s)], routed_hbm.at[:, side(s)], w_sem.at[18 + s])
        out.start()
        leaving.append(out)

    leaving = []

    key_scale = size**-0.5

    def summary():
        need(6, 7, 8, 9, 10)
        gate = fg_ref[...]
        keep = jnp.minimum(gate, 0.0) - jnp.log1p(jnp.exp(-jnp.abs(gate))) + fb_ref[...]
        upto = (iota((span, span), 0) <= iota((span, span), 1)).astype(f32)
        total = jnp.dot(
            stacked([keep], span), upto, preferred_element_type=f32, precision=lax.Precision.HIGHEST
        )[0:1]
        lead = ig_ref[...] - total
        last = total[:, span - 1 : span]
        top = jnp.max(last + lead, axis=1, keepdims=True)
        spread = jnp.exp(last + lead - top) * key_scale
        unit = (iota((8, 8), 0) == iota((8, 8), 1)).astype(f32)
        columns = lax.dot_general(
            stacked([total, spread], span),
            unit,
            (((0,), (0,)), ((), ())),
            preferred_element_type=f32,
            precision=lax.Precision.HIGHEST,
        )
        bcol_s[...] = columns[:, 0:1]
        weighted = k_ref[...].astype(f32) * columns[:, 1:2]
        ct[...] = dot_t(weighted.astype(bf16), v_ref[...])
        normer = jnp.sum(weighted, axis=0, keepdims=True)
        wide = jnp.zeros((1, size), f32)
        sm[...] = stacked([normer, last + wide, top + wide], size)
        for k in range(1, slab):
            place, device = slab_peer(k)
            for copy in s_copies(me, place, device):
                go(copy)
        sl[me] = ct[pl.ds(pl.multiple_of(me * piece, 8), piece), :]
        sm_all[me] = sm[...]
        lead_s[...] = lead

    def s_copies(src_place, dst_place, device):
        return (
            remote(
                ct.at[pl.ds(pl.multiple_of(dst_place * piece, 8), piece)],
                sl.at[src_place],
                s_send.at[0, dst_place],
                s_recv.at[0, src_place],
                device,
            ),
            remote(sm, sm_all.at[src_place], s_send.at[1, dst_place], s_recv.at[1, src_place], device),
        )

    def local():
        need(5)
        lead = lead_s[...]
        block = min(128, span)
        for at in range(0, span, block):
            end = at + block
            q = q_ref[at:end, :]
            products = dot_nt(q, k_ref[0:end, :]) * key_scale
            decay = bcol_s[at:end, :] + lead[:, 0:end]
            decay = jnp.where(iota((block, end), 1) <= iota((block, end), 0) + at, decay, floor_log)
            peak = jnp.max(decay, axis=1, keepdims=True)
            scores = products * jnp.exp(decay - peak)
            lpeak_s[at:end, :] = peak
            den_s[at:end, :] = jnp.sum(scores, axis=1, keepdims=True)
            num_loc[at:end, :] = dot(scores.astype(bf16), v_ref[0:end, :])

    def t_copies(src_z, k):
        return (
            remote(zs_out, zt.at[src_z], t_send.at[0, k], t_recv.at[0, src_z], z_peer(k)),
            remote(zm_out, zm.at[src_z], t_send.at[1, k], t_recv.at[1, src_z], z_peer(k)),
        )

    def unpacked(meta, memory):
        return (meta[1:2, :], meta[2:3, :], memory, meta[0:1, :])

    def nothing():
        zero = jnp.zeros((1, size), f32)
        return (zero, zero + floor_log, jnp.zeros((piece, size), f32), zero)

    def inside():
        for k in range(1, slab):
            place, device = slab_peer(k)
            for copy in s_copies(place, me, device):
                copy.wait_recv()
        state = nothing()
        for p in range(slab):
            ep_slice[p] = state[2]
            ep_meta[p] = stacked([state[3], state[0], state[1]], size)
            state = joined(state, unpacked(sm_all[p], sl[p]))
        zs_out[...] = state[2].astype(bf16)
        zm_out[...] = stacked([state[3], state[0], state[1]], size, 4)
        for k in (1, 7, 2, 6, 3, 5):
            for way, step in ways:
                arrived(min(k, NZ - k), 0, 0, way, step)
            for copy in t_copies(z, k):
                go(copy)

    def opposite_side():
        for way, step in ways:
            arrived(4, 0, 0, way, step)
        for copy in t_copies(z, 4):
            go(copy)

    def e_copy(src_place, dst_place, device):
        return remote(
            es.at[dst_place],
            ent.at[pl.ds(pl.multiple_of(src_place * piece, 16), piece)],
            e_send.at[dst_place],
            e_recv.at[src_place],
            device,
        )

    def across():
        for k in range(1, NZ):
            for copy in t_copies(lax.rem(z + k, NZ), NZ - k):
                copy.wait_recv()
        zt[z] = zs_out[...]
        zm[z] = zm_out[...]
        state = nothing()
        for s in range(NZ - 1):
            earlier = s < z
            total, peak, memory, normer = unpacked(zm[s], zt[s].astype(f32))
            part_of = (
                jnp.where(earlier, total, 0.0),
                jnp.where(earlier, peak, floor_log),
                jnp.where(earlier, memory, 0.0),
                jnp.where(earlier, normer, 0.0),
            )
            state = joined(state, part_of)
        for p in range(slab):
            es[p] = joined(state, unpacked(ep_meta[p], ep_slice[p]))[2].astype(bf16)
        for k in range(1, slab):
            place, device = slab_peer(k)
            go(e_copy(me, place, device))
        ent[pl.ds(pl.multiple_of(me * piece, 16), piece), :] = es[me]
        total, peak, _, normer = state
        both = joined((total, peak, None, normer), unpacked(ep_meta[me], None))
        into_s[...] = stacked([both[3], both[0], both[1]], size)

    def h_copy(src_y, dst_y, device):
        quarter = span // ny
        return remote(
            hs.at[pl.ds(pl.multiple_of(dst_y * quarter, 16), quarter)],
            hb.at[src_y],
            h_send.at[dst_y],
            h_recv.at[src_y],
            device,
        )

    def cells():
        need(11)
        _, stabil, _, normer = unpacked(into_s[...], None)
        for k in range(1, slab):
            place, device = slab_peer(k)
            e_copy(place, me, device).wait_recv()
        block = min(256, span)
        for at in range(0, span, block):
            end = at + block
            q = q_ref[at:end, :]
            carried = bcol_s[at:end, :] + stabil[:, 0:1]
            peak = jnp.maximum(carried, lpeak_s[at:end, :])
            factor = jnp.exp(lpeak_s[at:end, :] - peak)
            across_ = jnp.exp(carried - peak)
            den = factor * den_s[at:end, :] + across_ * jnp.sum(q.astype(f32) * normer, axis=1, keepdims=True)
            num = factor * num_loc[at:end, :] + across_ * dot(q, ent[...])
            cell = num / jnp.maximum(jnp.abs(den), jnp.exp(-peak))
            hs[at:end, :] = (cell * hscale_ref[...]).astype(bf16)
        quarter = span // ny
        for k in range(1, ny):
            place, device = y_peer(k)
            go(h_copy(yy, place, device))
        hb[yy] = hs[pl.ds(pl.multiple_of(yy * quarter, 16), quarter), :]

    def project():
        for k in range(1, ny):
            place, device = y_peer(k)
            h_copy(place, yy, device).wait_recv()
        need(12, 16)
        quarter = span // ny
        total = jnp.zeros((quarter, width), f32)
        for y in range(ny):
            total = total + dot(hb[y], wo[y * size : (y + 1) * size, :])
        squares = jnp.mean(total * total, axis=-1, keepdims=True)
        mixed_ref[...] = (total * lax.rsqrt(squares + norm_eps) * pscale_ref[...]).astype(bf16)
        out = pltpu.make_async_copy(mixed_ref, mixed_hbm, w_sem.at[17])
        out.start()
        leaving.append(out)

    steps = dict(
        S=send,
        pick=pick,
        gate=gate,
        give=give,
        weigh=weigh,
        P=pass_on,
        summary=summary,
        local=local,
        inside=inside,
        far=opposite_side,
        across=across,
        cells=cells,
        project=project,
        final=finish,
    )
    for line in ORDER.split():
        name, *numbers = line.split(",")
        steps[name](*(int(k) for k in numbers))
    for copy in pending:
        copy.wait_send()
    for copy in leaving:
        copy.wait()


def copied(a_ref, b_ref, a_out, b_out, a_held, b_held, sems):
    moves = []
    for n, (src, held, dst) in enumerate(((a_ref, a_held, a_out), (b_ref, b_held, b_out))):
        block = src.shape[0] // 2
        for k in range(2):
            at = pl.ds(k * block, block)
            into = pltpu.make_async_copy(src.at[at], held.at[at], sems.at[n, k, 0])
            into.start()
            moves.append((into, pltpu.make_async_copy(held.at[at], dst.at[at], sems.at[n, k, 1])))
    for into, out in moves:
        into.wait()
        out.start()
    for _, out in moves:
        out.wait()


def shards(
    memory_query_matrix,
    memory_key_matrix,
    memory_value_matrix,
    input_gate_logits,
    forget_gate_logits,
    forget_log_boosts,
    head_norm_scale,
    memory_output_matrix,
    projection_norm_scale,
    second_batch_rows,
    expert_prenorm_scale,
    selected_expert_index,
    group_route_probability,
    expert_choice_scores,
    expert_gate_matrix,
    expert_up_matrix,
    expert_down_matrix,
):
    nx, nc, ny = (lax.axis_size(a) for a in ("ep_1", "ep_2", "tp"))
    slab = nx * nc
    tokens, width = second_batch_rows.shape
    span, size = memory_query_matrix.shape
    hidden = expert_gate_matrix.shape[2]
    piece = size // slab
    part = tokens // 4
    cellw = memory_output_matrix.shape[0]
    most = slab * 2 * CAP
    anywhere = pl.BlockSpec(memory_space=pl.ANY)
    dma = pltpu.SemaphoreType.DMA
    rounds = len(ROUNDS)
    inputs = (
        second_batch_rows,
        selected_expert_index.T,
        group_route_probability[None, :],
        expert_choice_scores.T,
        expert_prenorm_scale[None, :],
        memory_query_matrix,
        memory_key_matrix,
        memory_value_matrix,
        input_gate_logits,
        forget_gate_logits,
        forget_log_boosts,
        head_norm_scale[None, :],
        projection_norm_scale[None, :],
        expert_gate_matrix,
        expert_up_matrix,
        expert_down_matrix,
        memory_output_matrix,
    )
    scratch = [pltpu.VMEM(a.shape[-2:], a.dtype) for a in inputs]
    scratch += [
        pltpu.VMEM((tokens, width), bf16),
        pltpu.VMEM((span // ny, width), bf16),
        pltpu.VMEM((tokens, width), bf16),
        pltpu.VMEM((rounds, most, hidden), bf16),
        pltpu.VMEM((1, span), f32),
        pltpu.VMEM((8, size), f32),
        pltpu.VMEM((2, tokens, width), bf16),
        pltpu.VMEM((2, tokens, tokens), bf16),
        pltpu.VMEM((8, tokens), f32),
        pltpu.VMEM((2, 8, tokens), bf16),
        pltpu.VMEM((2, 4, 8, tokens), bf16),
        pltpu.VMEM((2, 4, tokens, width), bf16),
        pltpu.VMEM((rounds, most, width), bf16),
        pltpu.VMEM((rounds, most, width), bf16),
        pltpu.VMEM((rounds, most, width), bf16),
        pltpu.VMEM((rounds, most, width), bf16),
        pltpu.VMEM((2, 4, tokens, width), bf16),
        pltpu.VMEM((2, 4, tokens, width), bf16),
        pltpu.VMEM((tokens, width), f32),
        pltpu.VMEM((size, size), f32),
        pltpu.VMEM((8, size), f32),
        pltpu.VMEM((slab, piece, size), f32),
        pltpu.VMEM((slab, 8, size), f32),
        pltpu.VMEM((piece, size), bf16),
        pltpu.VMEM((4, size), f32),
        pltpu.VMEM((NZ, piece, size), bf16),
        pltpu.VMEM((NZ, 4, size), f32),
        pltpu.VMEM((slab, piece, size), f32),
        pltpu.VMEM((slab, 8, size), f32),
        pltpu.VMEM((slab, piece, size), bf16),
        pltpu.VMEM((size, size), bf16),
        pltpu.VMEM((span, size), f32),
        pltpu.VMEM((span, 1), f32),
        pltpu.VMEM((span, 1), f32),
        pltpu.VMEM((span, 1), f32),
        pltpu.VMEM((span, size), bf16),
        pltpu.VMEM((ny, span // ny, size), bf16),
        dma((18 + HALVES,)),
        dma((2, 4)),
        dma((2, 4)),
        dma((2, 4, 4, 2)),
        dma((2, 4, 4, 2)),
        dma((2, 4, 4, HALVES)),
        dma((2, 4, 4, HALVES)),
        dma((rounds, slab, 2)),
        dma((rounds, slab, 2)),
        dma((rounds, slab, HALVES)),
        dma((rounds, slab, HALVES)),
        dma((2, slab)),
        dma((2, slab)),
        dma((2, NZ)),
        dma((2, NZ)),
        dma((slab,)),
        dma((slab,)),
        dma((ny,)),
        dma((ny,)),
    ]
    shapes = (
        jax.ShapeDtypeStruct((span // ny, width), bf16),
        jax.ShapeDtypeStruct((tokens, width), bf16),
    )
    mixed, routed = pl.pallas_call(
        functools.partial(body, (nx, nc, ny)),
        out_shape=shapes,
        in_specs=[anywhere] * len(inputs),
        out_specs=(anywhere, anywhere),
        scratch_shapes=scratch,
        compiler_params=pltpu.CompilerParams(
            collective_id=0, has_side_effects=True, vmem_limit_bytes=67043328
        ),
    )(*inputs)
    return pl.pallas_call(
        copied,
        out_shape=shapes,
        in_specs=[anywhere] * 2,
        out_specs=(anywhere, anywhere),
        scratch_shapes=[
            pltpu.VMEM(shapes[0].shape, bf16),
            pltpu.VMEM(shapes[1].shape, bf16),
            dma((2, 2, 2)),
        ],
    )(mixed, routed)


def solution(mesh):
    finer = Mesh(mesh.devices.reshape(8, 4, 2, mesh.shape["tp"]), EP_TP)
    in_specs = (
        P(EP, "tp"),
        P(EP, "tp"),
        P(EP, "tp"),
        P("tp", EP),
        P("tp", EP),
        P("tp", EP),
        P("tp"),
        P(),
        P(),
        P(EP_TP, None),
        P(),
        P(EP_TP, None),
        P(EP_TP),
        P(EP_TP, None),
        P(EP, None, None),
        P(EP, None, None),
        P(EP, None, None),
    )
    out_specs = (P(EP_TP, None), P(EP_TP, None))
    return jax.shard_map(shards, mesh=finer, in_specs=in_specs, out_specs=out_specs, check_vma=False)
```

```python
import functools

import jax
import jax.numpy as jnp
from jax import lax
from jax.experimental import pallas as pl
from jax.experimental.pallas import tpu as pltpu
from jax.sharding import Mesh
from jax.sharding import PartitionSpec as P

EP = ("ep_0", "ep_1", "ep_2")
EP_TP = ("ep_0", "ep_1", "ep_2", "tp")
NZ = 8
CAP = 12
SENT = (4, 4, 3, 1)
ORDER = """
S,1,0,1 S,1,1,0 S,1,3,0 S,1,0,0 S,1,2,0 pick,0,1 pick,0,0 S,1,1,1 S,1,3,1 gate,0 pick,1,0 S,1,2,1
S,2,2,0 S,2,3,0 S,2,1,0 S,2,0,0 summary pick,1,1 S,2,2,1 S,2,3,1 S,2,1,1 S,2,0,1 local S,3,0,0
pick,2,0 gate,1 give,1,1 S,3,2,0 pick,2,1 S,3,1,0 S,3,0,1 S,3,2,1 pick,3,0 S,3,1,1 S,4,0,0 weigh,1,1
gate,2 give,2,1 pick,3,1 give,2,0 weigh,2,1 inside P,2,3,1 S,4,0,1 gate,3 give,3,1 give,3,0 P,1,3,1
far pick,4,1 weigh,2,0 P,2,3,0 weigh,3,1 P,3,1,1 P,3,2,1 pick,4,0 P,2,1,1 weigh,3,0 P,3,1,0 give,1,0
P,3,2,0 P,2,2,1 gate,4 give,4,0 P,2,1,0 across P,1,1,1 weigh,1,0 give,4,1 P,1,2,1 give,0,1 P,1,3,0
P,2,2,0 weigh,4,1 give,0,0 weigh,4,0 P,4,0,0 P,4,0,1 cells P,1,1,0 P,3,0,0 project P,3,0,1 P,2,0,0
P,2,0,1 P,1,0,0 weigh,0,1 P,1,2,0 weigh,0,0 P,1,0,1 final,0 final,1
"""
HALVES = 2
ROUNDS = (0, 1, 4, 3, 2)

floor_log = -1e30
norm_eps = 1e-06
f32 = jnp.float32
bf16 = jnp.bfloat16
MESH = pl.DeviceIdType.MESH


def iota(shape, dim):
    return lax.broadcasted_iota(jnp.int32, shape, dim)


def dot(a, b):
    return jnp.dot(a, b, preferred_element_type=f32)


def dot_t(a, b):
    return lax.dot_general(a, b, (((0,), (0,)), ((), ())), preferred_element_type=f32)


def dot_nt(a, b):
    return lax.dot_general(a, b, (((1,), (1,)), ((), ())), preferred_element_type=f32)


def stacked(rows, width, count=8):
    place = iota((count, width), 0)
    out = jnp.zeros((count, width), f32)
    for k, row in enumerate(rows):
        out = jnp.where(place == k, row, out)
    return out


def joined(early, late):
    total_e, peak_e, memory_e, normer_e = early
    total_l, peak_l, memory_l, normer_l = late
    peak = jnp.maximum(total_l + peak_e, peak_l)
    factor_e = jnp.exp(total_l + peak_e - peak)
    factor_l = jnp.exp(peak_l - peak)
    memory = None if memory_e is None else factor_e * memory_e + factor_l * memory_l
    return (total_e + total_l, peak, memory, factor_e * normer_e + factor_l * normer_l)


def body(
    dims,
    *refs,
):
    given, made, (
        x_ref,
        ids_ref,
        prob_ref,
        score_ref,
        gain_ref,
        q_ref,
        k_ref,
        v_ref,
        ig_ref,
        fg_ref,
        fb_ref,
        hscale_ref,
        pscale_ref,
        wg,
        wu,
        wd,
        wo,
    ), mine = refs[:17], refs[17:19], refs[19:36], refs[36:]
    mixed_hbm, routed_hbm = made
    (
        xn,
        mixed_ref,
        routed_ref,
        hid,
        lead_s,
        into_s,
        xd,
        perm,
        own_meta,
        md,
        mz,
        dz,
        gb,
        rb,
        ob,
        yb,
        ts,
        tr,
        acc,
        ct,
        sm,
        sl,
        sm_all,
        zs_out,
        zm_out,
        zt,
        zm,
        ep_slice,
        ep_meta,
        es,
        ent,
        num_loc,
        lpeak_s,
        den_s,
        bcol_s,
        hs,
        hb,
        w_sem,
        meta_send,
        meta_recv,
        z_send,
        z_recv,
        b_send,
        b_recv,
        x_send,
        x_recv,
        y_send,
        y_recv,
        s_send,
        s_recv,
        t_send,
        t_recv,
        e_send,
        e_recv,
        h_send,
        h_recv,
    ) = mine
    nx, nc, ny = dims
    slab = nx * nc
    tokens, width = x_ref.shape
    part = tokens // 4
    span = q_ref.shape[0]
    size = q_ref.shape[1]
    piece = size // slab
    cols = min(512, width // HALVES)
    z, xx, cc, yy = (lax.axis_index(a) for a in EP_TP)
    me = xx * nc + cc

    def z_peer(step):
        return (lax.rem(z + step + NZ, NZ), xx, cc, yy)

    def slab_peer(k):
        place = lax.rem(me + k, slab)
        return place, (z, place // nc, lax.rem(place, nc), yy)

    def y_peer(k):
        place = lax.rem(yy + k, ny)
        return place, (z, xx, cc, place)

    others = slab - 1

    def drained(ref, sem):
        pltpu.make_async_copy(ref, ref, sem).wait()

    def remote(src, dst, send, recv, device):
        return pltpu.make_async_remote_copy(
            src_ref=src, dst_ref=dst, send_sem=send, recv_sem=recv, device_id=device, device_id_type=MESH
        )

    def go(copy):
        copy.start()

    barrier = pltpu.get_barrier_semaphore()
    greeted = [z_peer(1), z_peer(-1)]
    greeted += [slab_peer(k)[1] for k in range(1, slab)]
    greeted += [y_peer(k)[1] for k in range(1, ny)]
    for device in greeted:
        pl.semaphore_signal(barrier, inc=1, device_id=device, device_id_type=MESH)

    loads = []
    for k, (src, dst) in enumerate(zip(given, refs[19:36])):
        load = pltpu.make_async_copy(src.at[0] if len(src.shape) == 3 else src, dst, w_sem.at[k])
        load.start()
        loads.append(load)
    held = set()

    def need(*numbers):
        for k in numbers:
            if k not in held:
                held.add(k)
                loads[k].wait()

    need(0, 1, 2, 3, 4)

    rows = x_ref[...].astype(f32)
    squares = jnp.mean(rows * rows, axis=-1, keepdims=True)
    xn[...] = (rows * lax.rsqrt(squares + norm_eps) * gain_ref[...]).astype(bf16)

    experts = NZ * slab
    ids = ids_ref[...].astype(f32)
    e0, e1 = ids[0:1, :], ids[1:2, :]
    prob, s0, s1 = prob_ref[...], score_ref[0:1, :], score_ref[1:2, :]
    lanes = iota((experts, tokens), 0).astype(f32)
    oh0, oh1 = (e0 == lanes).astype(f32), (e1 == lanes).astype(f32)
    before = (iota((tokens, tokens), 0) < iota((tokens, tokens), 1)).astype(bf16)
    counts = dot((oh0 + oh1).astype(bf16), before)
    r0 = jnp.sum(counts * oh0, axis=0, keepdims=True)
    r1 = jnp.sum(counts * oh1, axis=0, keepdims=True)
    zf = z.astype(f32)

    def distance(e):
        d = jnp.floor(e * (1.0 / slab)) - zf
        return jnp.where(d < 0, d + NZ, d)

    def either(d):
        return jnp.where((d0 == d) | (d1 == d), 1.0, 0.0)

    d0, d1 = distance(e0), distance(e1)
    opposite = either(4)
    rank = dot(stacked([opposite], tokens).astype(bf16), before)[0:1]
    first = [jnp.where(rank < part, opposite, 0.0), jnp.where(rank < part, 0.0, opposite)]
    classes = []
    for way, far in ((0, 3), (1, 5)):
        second = either(far) * (1.0 - first[way])
        classes += [first[way], second, 1.0 - first[way] - second]
    ranks = dot(stacked(classes, tokens).astype(bf16), before)
    high = jnp.maximum(s0, s1)
    a0, a1 = jnp.exp(s0 - high), jnp.exp(s1 - high)
    w0, w1 = prob * a0 / (a0 + a1), prob * a1 / (a0 + a1)
    own_meta[...] = stacked([e0, r0, e1, r1, w0, w1], tokens)
    slots = iota((tokens, tokens), 0).astype(f32)
    for way in range(2):
        c0, c1, c2 = classes[3 * way : 3 * way + 3]
        n0 = jnp.sum(c0, axis=1, keepdims=True)
        n1 = jnp.sum(c1, axis=1, keepdims=True)
        place = (
            c0 * ranks[3 * way : 3 * way + 1]
            + c1 * (n0 + ranks[3 * way + 1 : 3 * way + 2])
            + c2 * (n0 + n1 + ranks[3 * way + 2 : 3 * way + 3])
        )
        order = (slots == place).astype(bf16)
        perm[way] = order
        other = first[1 - way] > 0.5
        f0 = jnp.where((d0 == 4) & other, 127.0, e0)
        f1 = jnp.where((d1 == 4) & other, 127.0, e1)
        table = stacked([f0, r0, f1, r1, w0, w1], tokens).astype(bf16)
        md[way] = dot_nt(table, order).astype(bf16)
        for n in range(0, width, cols):
            xd[way, :, n : n + cols] = dot(order, xn[:, n : n + cols]).astype(bf16)

    pl.semaphore_wait(barrier, len(greeted))

    ways = ((0, 1), (1, -1))

    def chunk(c):
        return pl.ds(c * part, part)

    there = width // 2

    def wing(d):
        return pl.ds(d * there, there)

    def outward(h, c, d, way, step):
        src = xd.at[way, chunk(c), wing(d)] if h == 1 else dz.at[way, h - 2, chunk(c), wing(d)]
        return remote(
            src,
            dz.at[way, h - 1, chunk(c), wing(d)],
            z_send.at[0],
            z_recv.at[way, sum(SENT[: h - 1]) + c, d],
            z_peer(step),
        )

    landed = set()
    spread = set()

    def arrived(h, c, d, way, step):
        if (h, c, d, way) not in landed:
            landed.add((h, c, d, way))
            outward(h, c, d, way, step).wait_recv()

    def send(h, c, d):
        for way, step in ways:
            if h > 1:
                arrived(h - 1, c, d, way, step)
            go(outward(h, c, d, way, step))
        if h not in spread:
            spread.add(h)
            known(h - 1)
            for way, step in ways:
                go(meta_copy(way, step, h))

    def meta_copy(way, step, h):
        some = pl.ds(0, tokens if h < 4 else min(tokens, 128))
        src = md.at[way, :, some] if h == 1 else mz.at[way, h - 2, :, some]
        return remote(
            src, mz.at[way, h - 1, :, some], meta_send.at[h // 4], meta_recv.at[way, h - 1], z_peer(step)
        )

    told = {}

    def known(h):
        if h and not told.setdefault(h, False):
            told[h] = True
            for way, step in ways:
                meta_copy(way, step, h).wait_recv()

    half = width // HALVES

    def side(s):
        return pl.ds(s * half, half)

    def homeward(h, c, s, way, step):
        return remote(
            ts.at[way, h - 1, chunk(c), side(s)],
            tr.at[way, h - 1, chunk(c), side(s)],
            b_send.at[0],
            b_recv.at[way, 0, s] if h == 1 else b_recv.at[way, 1 + sum(SENT[1 : h - 1]) + c, s],
            z_peer(-step),
        )

    def room(r):
        return 16 if r in (0, 4) else 2 * CAP

    def wanted(r, part_of):
        count = slab * room(r)
        at = iota((count, 1), 0)
        expert = jnp.zeros((count, 1), jnp.int32)
        for k in range(1, slab):
            expert = expert + jnp.where(at >= k * room(r), 1, 0)
        within = at - expert * room(r) - part_of * CAP
        good = (within >= 0) & (within < CAP)
        return jnp.where(good, (z * slab + expert) * CAP + within, -1).astype(f32)

    def streams(r):
        if r == 0:
            return [(own_meta, None, tokens, 0)]
        taken = SENT[r - 1] * part
        return [(mz.at[way, r - 1], way, taken, 0 if r == 4 else way) for way in range(2)]

    def chosen(meta, taken, want, weighted):
        k0 = meta[0:1, 0:taken] * CAP + meta[1:2, 0:taken]
        k1 = meta[2:3, 0:taken] * CAP + meta[3:4, 0:taken]
        if not weighted:
            return ((k0 == want) | (k1 == want)).astype(bf16)
        return (
            jnp.where(k0 == want, meta[4:5, 0:taken], 0.0) + jnp.where(k1 == want, meta[5:6, 0:taken], 0.0)
        ).astype(bf16)

    def x_copy(r, d, src_place, dst_place, device):
        rows_of = pl.ds(pl.multiple_of(dst_place * room(r), 8), room(r))
        lands = pl.ds(pl.multiple_of(src_place * room(r), 8), room(r))
        n = ROUNDS.index(r)
        return remote(
            gb.at[n, rows_of, wing(d)],
            rb.at[n, lands, wing(d)],
            x_send.at[r % 4 and 1],
            x_recv.at[n],
            device,
        )

    def y_copy(r, s, src_place, dst_place, device):
        rows_of = pl.ds(pl.multiple_of(dst_place * room(r), 8), room(r))
        lands = pl.ds(pl.multiple_of(src_place * room(r), 8), room(r))
        n = ROUNDS.index(r)
        return remote(
            ob.at[n, rows_of, side(s)],
            yb.at[n, lands, side(s)],
            y_send.at[r % 4 and 1],
            y_recv.at[n, s],
            device,
        )

    def pick(r, d):
        n, count = ROUNDS.index(r), slab * room(r)
        known(r)
        for c in range(SENT[r - 1] if r else 0):
            for way, step in ways:
                arrived(r, c, d, way, step)
        picks = []
        for meta, way, taken, second in streams(r):
            picks.append((chosen(meta[...].astype(f32), taken, wanted(r, second), False), way, taken))

        @pl.loop(0, there // cols)
        def _(t):
            at = pl.ds(pl.multiple_of(d * there + t * cols, 128), cols)
            total = jnp.zeros((count, cols), f32)
            for one_hot, way, taken in picks:
                source = xn[0:taken, at] if way is None else dz[way, r - 1, 0:taken, at]
                total = total + dot(one_hot, source)
            gb[n, 0:count, at] = total.astype(bf16)

        for k in range(1, slab):
            place, device = slab_peer(k)
            go(x_copy(r, d, me, place, device))
        own = pl.ds(pl.multiple_of(me * room(r), 8), room(r))
        rb[n, own, wing(d)] = gb[n, own, wing(d)]

    def gate(r):
        n, count = ROUNDS.index(r), slab * room(r)
        if others:
            drained(rb.at[n, pl.ds(0, others * room(r))], x_recv.at[n])
        need(13, 14)
        rows = rb[n, 0:count, :]
        value = dot(rows, wg[...])
        hid[n, 0:count, :] = (value / (1.0 + jnp.exp(-value)) * dot(rows, wu[...])).astype(bf16)

    def give(r, s):
        n, count = ROUNDS.index(r), slab * room(r)
        need(15)
        hidden = hid[n, 0:count, :]

        @pl.loop(0, half // cols)
        def _(t):
            at = pl.ds(pl.multiple_of(s * half + t * cols, 128), cols)
            ob[n, 0:count, at] = dot(hidden, wd[:, at]).astype(bf16)

        for k in range(1, slab):
            place, device = slab_peer(k)
            go(y_copy(r, s, me, place, device))
        own = pl.ds(pl.multiple_of(me * room(r), 8), room(r))
        yb[n, own, side(s)] = ob[n, own, side(s)]

    def weigh(r, s):
        n, count = ROUNDS.index(r), slab * room(r)
        if others:
            drained(yb.at[n, pl.ds(0, others * room(r)), side(s)], y_recv.at[n, s])
        parts = []
        for meta, way, taken, second in streams(r):
            parts.append((chosen(meta[...].astype(f32), taken, wanted(r, second), True), way, taken))

        @pl.loop(0, half // cols)
        def _(t):
            at = pl.ds(pl.multiple_of(s * half + t * cols, 128), cols)
            for weights, way, taken in parts:
                value = dot_t(weights, yb[n, 0:count, at])
                if way is None:
                    acc[:, at] = value
                else:
                    ts[way, r - 1, 0:taken, at] = value.astype(bf16)

    def pass_on(h, c, s):
        for way, step in ways:
            if h < 4 and c < SENT[h]:
                homeward(h + 1, c, s, way, step).wait_recv()
                at = slice(c * part, (c + 1) * part)
                ts[way, h - 1, at, side(s)] = (
                    ts[way, h - 1, at, side(s)].astype(f32) + tr[way, h, at, side(s)].astype(f32)
                ).astype(bf16)
            go(homeward(h, c, s, way, step))

    def finish(s):
        for way in range(2):
            drained(tr.at[way, 0, :, side(s)], b_recv.at[way, 0, s])

        @pl.loop(0, half // cols)
        def _(t):
            at = pl.ds(pl.multiple_of(s * half + t * cols, 128), cols)
            total = acc[:, at]
            for way in range(2):
                total = total + dot_t(perm[way], tr[way, 0, :, at])
            routed_ref[:, at] = total.astype(bf16)

        out = pltpu.make_async_copy(routed_ref.at[:, side(s)], routed_hbm.at[:, side(s)], w_sem.at[18 + s])
        out.start()
        leaving.append(out)

    leaving = []

    key_scale = size**-0.5

    def summary():
        need(6, 7, 8, 9, 10)
        gate = fg_ref[...]
        keep = jnp.minimum(gate, 0.0) - jnp.log1p(jnp.exp(-jnp.abs(gate))) + fb_ref[...]
        upto = (iota((span, span), 0) <= iota((span, span), 1)).astype(f32)
        total = jnp.dot(
            stacked([keep], span), upto, preferred_element_type=f32, precision=lax.Precision.HIGHEST
        )[0:1]
        lead = ig_ref[...] - total
        last = total[:, span - 1 : span]
        top = jnp.max(last + lead, axis=1, keepdims=True)
        spread = jnp.exp(last + lead - top) * key_scale
        unit = (iota((8, 8), 0) == iota((8, 8), 1)).astype(f32)
        columns = lax.dot_general(
            stacked([total, spread], span),
            unit,
            (((0,), (0,)), ((), ())),
            preferred_element_type=f32,
            precision=lax.Precision.HIGHEST,
        )
        bcol_s[...] = columns[:, 0:1]
        weighted = k_ref[...].astype(f32) * columns[:, 1:2]
        ct[...] = dot_t(weighted.astype(bf16), v_ref[...])
        normer = jnp.sum(weighted, axis=0, keepdims=True)
        wide = jnp.zeros((1, size), f32)
        sm[...] = stacked([normer, last + wide, top + wide], size)
        for k in range(1, slab):
            place, device = slab_peer(k)
            for copy in s_copies(me, place, device):
                go(copy)
        sl[me] = ct[pl.ds(pl.multiple_of(me * piece, 8), piece), :]
        sm_all[me] = sm[...]
        lead_s[...] = lead

    def s_copies(src_place, dst_place, device):
        return (
            remote(
                ct.at[pl.ds(pl.multiple_of(dst_place * piece, 8), piece)],
                sl.at[src_place],
                s_send.at[0],
                s_recv.at[0],
                device,
            ),
            remote(sm, sm_all.at[src_place], s_send.at[1], s_recv.at[1], device),
        )

    def local():
        need(5)
        lead = lead_s[...]
        block = min(128, span)
        for at in range(0, span, block):
            end = at + block
            q = q_ref[at:end, :]
            products = dot_nt(q, k_ref[0:end, :]) * key_scale
            decay = bcol_s[at:end, :] + lead[:, 0:end]
            decay = jnp.where(iota((block, end), 1) <= iota((block, end), 0) + at, decay, floor_log)
            peak = jnp.max(decay, axis=1, keepdims=True)
            scores = products * jnp.exp(decay - peak)
            lpeak_s[at:end, :] = peak
            den_s[at:end, :] = jnp.sum(scores, axis=1, keepdims=True)
            num_loc[at:end, :] = dot(scores.astype(bf16), v_ref[0:end, :])

    def t_copies(src_z, k):
        return (
            remote(zs_out, zt.at[src_z], t_send.at[0], t_recv.at[0], z_peer(k)),
            remote(zm_out, zm.at[src_z], t_send.at[1], t_recv.at[1], z_peer(k)),
        )

    def unpacked(meta, memory):
        return (meta[1:2, :], meta[2:3, :], memory, meta[0:1, :])

    def nothing():
        zero = jnp.zeros((1, size), f32)
        return (zero, zero + floor_log, jnp.zeros((piece, size), f32), zero)

    def inside():
        if others:
            drained(sl.at[pl.ds(0, others)], s_recv.at[0])
            drained(sm_all.at[pl.ds(0, others)], s_recv.at[1])
        state = nothing()
        for p in range(slab):
            ep_slice[p] = state[2]
            ep_meta[p] = stacked([state[3], state[0], state[1]], size)
            state = joined(state, unpacked(sm_all[p], sl[p]))
        zs_out[...] = state[2].astype(bf16)
        zm_out[...] = stacked([state[3], state[0], state[1]], size, 4)
        for k in (1, 7, 2, 6, 3, 5):
            for way, step in ways:
                arrived(min(k, NZ - k), 0, 0, way, step)
            for copy in t_copies(z, k):
                go(copy)

    def opposite_side():
        for way, step in ways:
            arrived(4, 0, 0, way, step)
        for copy in t_copies(z, 4):
            go(copy)

    def e_copy(src_place, dst_place, device):
        return remote(
            es.at[dst_place],
            ent.at[pl.ds(pl.multiple_of(src_place * piece, 16), piece)],
            e_send.at[0],
            e_recv.at[0],
            device,
        )

    def across():
        drained(zt.at[pl.ds(0, NZ - 1)], t_recv.at[0])
        drained(zm.at[pl.ds(0, NZ - 1)], t_recv.at[1])
        zt[z] = zs_out[...]
        zm[z] = zm_out[...]
        state = nothing()
        for s in range(NZ - 1):
            earlier = s < z
            total, peak, memory, normer = unpacked(zm[s], zt[s].astype(f32))
            part_of = (
                jnp.where(earlier, total, 0.0),
                jnp.where(earlier, peak, floor_log),
                jnp.where(earlier, memory, 0.0),
                jnp.where(earlier, normer, 0.0),
            )
            state = joined(state, part_of)
        for p in range(slab):
            es[p] = joined(state, unpacked(ep_meta[p], ep_slice[p]))[2].astype(bf16)
        for k in range(1, slab):
            place, device = slab_peer(k)
            go(e_copy(me, place, device))
        ent[pl.ds(pl.multiple_of(me * piece, 16), piece), :] = es[me]
        total, peak, _, normer = state
        both = joined((total, peak, None, normer), unpacked(ep_meta[me], None))
        into_s[...] = stacked([both[3], both[0], both[1]], size)

    def h_copy(src_y, dst_y, device):
        quarter = span // ny
        return remote(
            hs.at[pl.ds(pl.multiple_of(dst_y * quarter, 16), quarter)],
            hb.at[src_y],
            h_send.at[0],
            h_recv.at[0],
            device,
        )

    def cells():
        need(11)
        _, stabil, _, normer = unpacked(into_s[...], None)
        if others:
            drained(ent.at[pl.ds(0, others * piece)], e_recv.at[0])
        block = min(256, span)
        for at in range(0, span, block):
            end = at + block
            q = q_ref[at:end, :]
            carried = bcol_s[at:end, :] + stabil[:, 0:1]
            peak = jnp.maximum(carried, lpeak_s[at:end, :])
            factor = jnp.exp(lpeak_s[at:end, :] - peak)
            across_ = jnp.exp(carried - peak)
            den = factor * den_s[at:end, :] + across_ * jnp.sum(q.astype(f32) * normer, axis=1, keepdims=True)
            num = factor * num_loc[at:end, :] + across_ * dot(q, ent[...])
            cell = num / jnp.maximum(jnp.abs(den), jnp.exp(-peak))
            hs[at:end, :] = (cell * hscale_ref[...]).astype(bf16)
        quarter = span // ny
        for k in range(1, ny):
            place, device = y_peer(k)
            go(h_copy(yy, place, device))
        hb[yy] = hs[pl.ds(pl.multiple_of(yy * quarter, 16), quarter), :]

    def project():
        if ny > 1:
            drained(hb.at[pl.ds(0, ny - 1)], h_recv.at[0])
        need(12, 16)
        quarter = span // ny
        total = jnp.zeros((quarter, width), f32)
        for y in range(ny):
            total = total + dot(hb[y], wo[y * size : (y + 1) * size, :])
        squares = jnp.mean(total * total, axis=-1, keepdims=True)
        mixed_ref[...] = (total * lax.rsqrt(squares + norm_eps) * pscale_ref[...]).astype(bf16)
        out = pltpu.make_async_copy(mixed_ref, mixed_hbm, w_sem.at[17])
        out.start()
        leaving.append(out)

    steps = dict(
        S=send,
        pick=pick,
        gate=gate,
        give=give,
        weigh=weigh,
        P=pass_on,
        summary=summary,
        local=local,
        inside=inside,
        far=opposite_side,
        across=across,
        cells=cells,
        project=project,
        final=finish,
    )
    for line in ORDER.split():
        name, *numbers = line.split(",")
        steps[name](*(int(k) for k in numbers))
    drained(mz.at[:, pl.ds(0, 3)], meta_send.at[0])
    drained(mz.at[:, 3, :, pl.ds(0, min(tokens, 128))], meta_send.at[1])
    drained(dz.at[:, pl.ds(0, 3)], z_send.at[0])
    drained(tr.at[:, pl.ds(0, 3)], b_send.at[0])
    drained(zt.at[pl.ds(0, NZ - 1)], t_send.at[0])
    drained(zm.at[pl.ds(0, NZ - 1)], t_send.at[1])
    if others:
        for sems, held_in in ((x_send, gb), (y_send, yb)):
            drained(held_in.at[pl.ds(0, 2), pl.ds(0, others * room(0))], sems.at[0])
            drained(held_in.at[pl.ds(0, 3), pl.ds(0, others * room(1))], sems.at[1])
        drained(sl.at[pl.ds(0, others)], s_send.at[0])
        drained(sm_all.at[pl.ds(0, others)], s_send.at[1])
        drained(es.at[pl.ds(0, others)], e_send.at[0])
    if ny > 1:
        drained(hb.at[pl.ds(0, ny - 1)], h_send.at[0])
    for copy in leaving:
        copy.wait()


def copied(a_ref, b_ref, a_out, b_out, a_held, b_held, sems):
    moves = []
    for n, (src, held, dst) in enumerate(((a_ref, a_held, a_out), (b_ref, b_held, b_out))):
        block = src.shape[0] // 2
        for k in range(2):
            at = pl.ds(k * block, block)
            into = pltpu.make_async_copy(src.at[at], held.at[at], sems.at[n, k, 0])
            into.start()
            moves.append((into, pltpu.make_async_copy(held.at[at], dst.at[at], sems.at[n, k, 1])))
    for into, out in moves:
        into.wait()
        out.start()
    for _, out in moves:
        out.wait()


def shards(
    memory_query_matrix,
    memory_key_matrix,
    memory_value_matrix,
    input_gate_logits,
    forget_gate_logits,
    forget_log_boosts,
    head_norm_scale,
    memory_output_matrix,
    projection_norm_scale,
    second_batch_rows,
    expert_prenorm_scale,
    selected_expert_index,
    group_route_probability,
    expert_choice_scores,
    expert_gate_matrix,
    expert_up_matrix,
    expert_down_matrix,
):
    nx, nc, ny = (lax.axis_size(a) for a in ("ep_1", "ep_2", "tp"))
    slab = nx * nc
    tokens, width = second_batch_rows.shape
    span, size = memory_query_matrix.shape
    hidden = expert_gate_matrix.shape[2]
    piece = size // slab
    part = tokens // 4
    cellw = memory_output_matrix.shape[0]
    most = slab * 2 * CAP
    anywhere = pl.BlockSpec(memory_space=pl.ANY)
    dma = pltpu.SemaphoreType.DMA
    rounds = len(ROUNDS)
    inputs = (
        second_batch_rows,
        selected_expert_index.T,
        group_route_probability[None, :],
        expert_choice_scores.T,
        expert_prenorm_scale[None, :],
        memory_query_matrix,
        memory_key_matrix,
        memory_value_matrix,
        input_gate_logits,
        forget_gate_logits,
        forget_log_boosts,
        head_norm_scale[None, :],
        projection_norm_scale[None, :],
        expert_gate_matrix,
        expert_up_matrix,
        expert_down_matrix,
        memory_output_matrix,
    )
    scratch = [pltpu.VMEM(a.shape[-2:], a.dtype) for a in inputs]
    scratch += [
        pltpu.VMEM((tokens, width), bf16),
        pltpu.VMEM((span // ny, width), bf16),
        pltpu.VMEM((tokens, width), bf16),
        pltpu.VMEM((rounds, most, hidden), bf16),
        pltpu.VMEM((1, span), f32),
        pltpu.VMEM((8, size), f32),
        pltpu.VMEM((2, tokens, width), bf16),
        pltpu.VMEM((2, tokens, tokens), bf16),
        pltpu.VMEM((8, tokens), f32),
        pltpu.VMEM((2, 8, tokens), bf16),
        pltpu.VMEM((2, 4, 8, tokens), bf16),
        pltpu.VMEM((2, 4, tokens, width), bf16),
        pltpu.VMEM((rounds, most, width), bf16),
        pltpu.VMEM((rounds, most, width), bf16),
        pltpu.VMEM((rounds, most, width), bf16),
        pltpu.VMEM((rounds, most, width), bf16),
        pltpu.VMEM((2, 4, tokens, width), bf16),
        pltpu.VMEM((2, 4, tokens, width), bf16),
        pltpu.VMEM((tokens, width), f32),
        pltpu.VMEM((size, size), f32),
        pltpu.VMEM((8, size), f32),
        pltpu.VMEM((slab, piece, size), f32),
        pltpu.VMEM((slab, 8, size), f32),
        pltpu.VMEM((piece, size), bf16),
        pltpu.VMEM((4, size), f32),
        pltpu.VMEM((NZ, piece, size), bf16),
        pltpu.VMEM((NZ, 4, size), f32),
        pltpu.VMEM((slab, piece, size), f32),
        pltpu.VMEM((slab, 8, size), f32),
        pltpu.VMEM((slab, piece, size), bf16),
        pltpu.VMEM((size, size), bf16),
        pltpu.VMEM((span, size), f32),
        pltpu.VMEM((span, 1), f32),
        pltpu.VMEM((span, 1), f32),
        pltpu.VMEM((span, 1), f32),
        pltpu.VMEM((span, size), bf16),
        pltpu.VMEM((ny, span // ny, size), bf16),
        dma((18 + HALVES,)),
        dma((2,)),
        dma((2, 4)),
        dma((1,)),
        dma((2, sum(SENT), 2)),
        dma((1,)),
        dma((2, 1 + sum(SENT[1:]), HALVES)),
        dma((2,)),
        dma((rounds,)),
        dma((2,)),
        dma((rounds, HALVES)),
        dma((2,)),
        dma((2,)),
        dma((2,)),
        dma((2,)),
        dma((1,)),
        dma((1,)),
        dma((1,)),
        dma((1,)),
    ]
    shapes = (
        jax.ShapeDtypeStruct((span // ny, width), bf16),
        jax.ShapeDtypeStruct((tokens, width), bf16),
    )
    mixed, routed = pl.pallas_call(
        functools.partial(body, (nx, nc, ny)),
        out_shape=shapes,
        in_specs=[anywhere] * len(inputs),
        out_specs=(anywhere, anywhere),
        scratch_shapes=scratch,
        compiler_params=pltpu.CompilerParams(
            collective_id=0, has_side_effects=True, vmem_limit_bytes=67043328
        ),
    )(*inputs)
    return pl.pallas_call(
        copied,
        out_shape=shapes,
        in_specs=[anywhere] * 2,
        out_specs=(anywhere, anywhere),
        scratch_shapes=[
            pltpu.VMEM(shapes[0].shape, bf16),
            pltpu.VMEM(shapes[1].shape, bf16),
            dma((2, 2, 2)),
        ],
    )(mixed, routed)


def solution(mesh):
    finer = Mesh(mesh.devices.reshape(8, 4, 2, mesh.shape["tp"]), EP_TP)
    in_specs = (
        P(EP, "tp"),
        P(EP, "tp"),
        P(EP, "tp"),
        P("tp", EP),
        P("tp", EP),
        P("tp", EP),
        P("tp"),
        P(),
        P(),
        P(EP_TP, None),
        P(),
        P(EP_TP, None),
        P(EP_TP),
        P(EP_TP, None),
        P(EP, None, None),
        P(EP, None, None),
        P(EP, None, None),
    )
    out_specs = (P(EP_TP, None), P(EP_TP, None))
    return jax.shard_map(shards, mesh=finer, in_specs=in_specs, out_specs=out_specs, check_vma=False)
```

```python
import functools

import jax
import jax.numpy as jnp
from jax import lax
from jax.experimental import pallas as pl
from jax.experimental.pallas import tpu as pltpu
from jax.sharding import Mesh
from jax.sharding import PartitionSpec as P

EP = ("ep_0", "ep_1", "ep_2")
EP_TP = ("ep_0", "ep_1", "ep_2", "tp")
NZ = 8
CAP = 12
SENT = (4, 4, 3, 1)
ORDER = """
S,1,1,0 S,1,0,0 S,1,3,0 S,1,2,0 S,1,1,1 S,1,0,1 S,1,3,1 pick,0,0 S,1,2,1 pick,0,1 S,2,1,0 gate,0
S,2,2,0 S,2,0,0 give,0,2 give,0,0 S,2,3,0 pick,1,0 S,2,0,1 summary S,2,2,1 give,0,1 pick,1,1 S,2,3,1
S,2,1,1 pick,2,0 S,3,0,0 gate,1 give,1,3 give,1,1 S,3,1,0 S,3,2,0 pick,2,1 weigh,1,3 S,3,1,1 S,3,0,1
give,1,0 local pick,3,0 S,3,2,1 gate,2 S,4,0,0 weigh,1,1 give,2,0 pick,3,1 S,4,0,1 weigh,0,0 give,2,1
give,2,3 weigh,2,0 P,2,3,0 weigh,1,0 P,1,3,0 inside gate,3 give,3,1 give,3,3 weigh,2,1 P,2,3,1 give,3,0
far pick,4,0 weigh,2,3 give,0,3 P,2,3,3 weigh,0,1 pick,4,1 P,1,3,1 weigh,3,1 P,3,2,1 weigh,0,2 P,3,1,1
P,1,3,3 weigh,3,3 give,3,2 P,2,2,1 P,3,1,3 weigh,3,0 P,3,2,3 P,3,2,0 give,2,2 P,3,1,0 P,2,2,3 P,2,1,1
P,2,1,3 P,1,2,3 gate,4 P,2,1,0 give,4,2 give,4,1 weigh,3,2 P,3,1,2 P,2,2,0 P,1,1,3 across P,1,1,0
weigh,4,2 P,4,0,2 give,4,0 give,4,3 P,1,1,1 P,3,2,2 weigh,2,2 P,3,0,2 weigh,0,3 weigh,4,1 P,2,1,2 give,1,2
P,2,3,2 P,4,0,1 weigh,4,0 P,4,0,0 cells P,2,2,2 weigh,4,3 P,1,2,1 weigh,1,2 P,3,0,1 P,4,0,3 P,3,0,0
P,2,0,1 P,2,0,2 P,3,0,3 project P,1,2,2 P,2,0,0 P,2,0,3 P,1,0,2 P,1,0,0 P,1,0,1 P,1,3,2 P,1,0,3
P,1,1,2 P,1,2,0 final,1 final,3 final,2 final,0
"""
HALVES = 4
WINGS = 2
ROUNDS = (0, 1, 4, 3, 2)

floor_log = -1e30
norm_eps = 1e-06
f32 = jnp.float32
bf16 = jnp.bfloat16
MESH = pl.DeviceIdType.MESH


def iota(shape, dim):
    return lax.broadcasted_iota(jnp.int32, shape, dim)


def dot(a, b):
    return jnp.dot(a, b, preferred_element_type=f32)


def dot_t(a, b):
    return lax.dot_general(a, b, (((0,), (0,)), ((), ())), preferred_element_type=f32)


def dot_nt(a, b):
    return lax.dot_general(a, b, (((1,), (1,)), ((), ())), preferred_element_type=f32)


def stacked(rows, width, count=8):
    place = iota((count, width), 0)
    out = jnp.zeros((count, width), f32)
    for k, row in enumerate(rows):
        out = jnp.where(place == k, row, out)
    return out


def joined(early, late):
    total_e, peak_e, memory_e, normer_e = early
    total_l, peak_l, memory_l, normer_l = late
    peak = jnp.maximum(total_l + peak_e, peak_l)
    factor_e = jnp.exp(total_l + peak_e - peak)
    factor_l = jnp.exp(peak_l - peak)
    memory = None if memory_e is None else factor_e * memory_e + factor_l * memory_l
    return (total_e + total_l, peak, memory, factor_e * normer_e + factor_l * normer_l)


def body(
    dims,
    *refs,
):
    given, made, (
        x_ref,
        ids_ref,
        prob_ref,
        score_ref,
        gain_ref,
        q_ref,
        k_ref,
        v_ref,
        ig_ref,
        fg_ref,
        fb_ref,
        hscale_ref,
        pscale_ref,
        wg,
        wu,
        wd,
        wo,
    ), mine = refs[:17], refs[17:19], refs[19:36], refs[36:]
    mixed_hbm, routed_hbm = made
    (
        xn,
        mixed_ref,
        routed_ref,
        hid,
        lead_s,
        into_s,
        xd,
        perm,
        own_meta,
        md,
        mz,
        dz,
        gb,
        rb,
        ob,
        yb,
        ts,
        tr,
        acc,
        ct,
        sm,
        sl,
        sm_all,
        zs_out,
        zm_out,
        zt,
        zm,
        ep_slice,
        ep_meta,
        es,
        ent,
        num_loc,
        lpeak_s,
        den_s,
        bcol_s,
        hs,
        hb,
        w_sem,
        meta_send,
        meta_recv,
        z_send,
        z_recv,
        b_send,
        b_recv,
        x_send,
        x_recv,
        y_send,
        y_recv,
        s_send,
        s_recv,
        t_send,
        t_recv,
        e_send,
        e_recv,
        h_send,
        h_recv,
    ) = mine
    nx, nc, ny = dims
    slab = nx * nc
    tokens, width = x_ref.shape
    part = tokens // 4
    span = q_ref.shape[0]
    size = q_ref.shape[1]
    piece = size // slab
    cols = min(512, width // HALVES, width // WINGS)
    z, xx, cc, yy = (lax.axis_index(a) for a in EP_TP)
    me = xx * nc + cc

    def z_peer(step):
        return (lax.rem(z + step + NZ, NZ), xx, cc, yy)

    def slab_peer(k):
        place = lax.rem(me + k, slab)
        return place, (z, place // nc, lax.rem(place, nc), yy)

    def y_peer(k):
        place = lax.rem(yy + k, ny)
        return place, (z, xx, cc, place)

    others = slab - 1

    def drained(ref, sem):
        pltpu.make_async_copy(ref, ref, sem).wait()

    def remote(src, dst, send, recv, device):
        return pltpu.make_async_remote_copy(
            src_ref=src, dst_ref=dst, send_sem=send, recv_sem=recv, device_id=device, device_id_type=MESH
        )

    def go(copy):
        copy.start()

    barrier = pltpu.get_barrier_semaphore()
    greeted = [z_peer(1), z_peer(-1)]
    greeted += [slab_peer(k)[1] for k in range(1, slab)]
    greeted += [y_peer(k)[1] for k in range(1, ny)]
    for device in greeted:
        pl.semaphore_signal(barrier, inc=1, device_id=device, device_id_type=MESH)

    loads = []
    for k, (src, dst) in enumerate(zip(given, refs[19:36])):
        load = pltpu.make_async_copy(src.at[0] if len(src.shape) == 3 else src, dst, w_sem.at[k])
        load.start()
        loads.append(load)
    held = set()

    def need(*numbers):
        for k in numbers:
            if k not in held:
                held.add(k)
                loads[k].wait()

    need(0, 1, 2, 3, 4)

    rows = x_ref[...].astype(f32)
    squares = jnp.mean(rows * rows, axis=-1, keepdims=True)
    xn[...] = (rows * lax.rsqrt(squares + norm_eps) * gain_ref[...]).astype(bf16)

    experts = NZ * slab
    ids = ids_ref[...].astype(f32)
    e0, e1 = ids[0:1, :], ids[1:2, :]
    prob, s0, s1 = prob_ref[...], score_ref[0:1, :], score_ref[1:2, :]
    lanes = iota((experts, tokens), 0).astype(f32)
    oh0, oh1 = (e0 == lanes).astype(f32), (e1 == lanes).astype(f32)
    before = (iota((tokens, tokens), 0) < iota((tokens, tokens), 1)).astype(bf16)
    counts = dot((oh0 + oh1).astype(bf16), before)
    r0 = jnp.sum(counts * oh0, axis=0, keepdims=True)
    r1 = jnp.sum(counts * oh1, axis=0, keepdims=True)
    zf = z.astype(f32)

    def distance(e):
        d = jnp.floor(e * (1.0 / slab)) - zf
        return jnp.where(d < 0, d + NZ, d)

    def either(d):
        return jnp.where((d0 == d) | (d1 == d), 1.0, 0.0)

    d0, d1 = distance(e0), distance(e1)
    opposite = either(4)
    rank = dot(stacked([opposite], tokens).astype(bf16), before)[0:1]
    first = [jnp.where(rank < part, opposite, 0.0), jnp.where(rank < part, 0.0, opposite)]
    classes = []
    for way, far in ((0, 3), (1, 5)):
        second = either(far) * (1.0 - first[way])
        classes += [first[way], second, 1.0 - first[way] - second]
    ranks = dot(stacked(classes, tokens).astype(bf16), before)
    high = jnp.maximum(s0, s1)
    a0, a1 = jnp.exp(s0 - high), jnp.exp(s1 - high)
    w0, w1 = prob * a0 / (a0 + a1), prob * a1 / (a0 + a1)
    own_meta[...] = stacked([e0, r0, e1, r1, w0, w1], tokens)
    slots = iota((tokens, tokens), 0).astype(f32)
    for way in range(2):
        c0, c1, c2 = classes[3 * way : 3 * way + 3]
        n0 = jnp.sum(c0, axis=1, keepdims=True)
        n1 = jnp.sum(c1, axis=1, keepdims=True)
        place = (
            c0 * ranks[3 * way : 3 * way + 1]
            + c1 * (n0 + ranks[3 * way + 1 : 3 * way + 2])
            + c2 * (n0 + n1 + ranks[3 * way + 2 : 3 * way + 3])
        )
        order = (slots == place).astype(bf16)
        perm[way] = order
        other = first[1 - way] > 0.5
        f0 = jnp.where((d0 == 4) & other, 127.0, e0)
        f1 = jnp.where((d1 == 4) & other, 127.0, e1)
        table = stacked([f0, r0, f1, r1, w0, w1], tokens).astype(bf16)
        md[way] = dot_nt(table, order).astype(bf16)
        for n in range(0, width, cols):
            xd[way, :, n : n + cols] = dot(order, xn[:, n : n + cols]).astype(bf16)

    pl.semaphore_wait(barrier, len(greeted))

    ways = ((0, 1), (1, -1))

    def chunk(c):
        return pl.ds(c * part, part)

    there = width // WINGS

    def wing(d):
        return pl.ds(d * there, there)

    def outward(h, c, d, way, step):
        src = xd.at[way, chunk(c), wing(d)] if h == 1 else dz.at[way, h - 2, chunk(c), wing(d)]
        return remote(
            src,
            dz.at[way, h - 1, chunk(c), wing(d)],
            z_send.at[0],
            z_recv.at[sum(SENT[: h - 1]) + c, d],
            z_peer(step),
        )

    landed = set()
    spread = set()

    def arrived(h, c, d):
        if (h, c, d) not in landed:
            landed.add((h, c, d))
            drained(dz.at[:, h - 1, chunk(c), wing(d)], z_recv.at[sum(SENT[: h - 1]) + c, d])

    def send(h, c, d):
        if h > 1:
            arrived(h - 1, c, d)
        for way, step in ways:
            go(outward(h, c, d, way, step))
        if h not in spread:
            spread.add(h)
            known(h - 1)
            for way, step in ways:
                go(meta_copy(way, step, h))

    def meta_copy(way, step, h):
        some = pl.ds(0, tokens if h < 4 else min(tokens, 128))
        src = md.at[way, :, some] if h == 1 else mz.at[way, h - 2, :, some]
        return remote(
            src, mz.at[way, h - 1, :, some], meta_send.at[h // 4], meta_recv.at[h - 1], z_peer(step)
        )

    told = {}

    def known(h):
        if h and not told.setdefault(h, False):
            told[h] = True
            drained(mz.at[:, h - 1, :, pl.ds(0, tokens if h < 4 else min(tokens, 128))], meta_recv.at[h - 1])

    half = width // HALVES

    def side(s):
        return pl.ds(s * half, half)

    def homeward(h, c, s, way, step):
        return remote(
            ts.at[way, h - 1, chunk(c), side(s)],
            tr.at[way, h - 1, chunk(c), side(s)],
            b_send.at[0],
            b_recv.at[0 if h == 1 else 1 + sum(SENT[1 : h - 1]) + c, s],
            z_peer(-step),
        )

    def room(r):
        return 16 if r in (0, 4) else 2 * CAP

    def wanted(r, part_of):
        count = slab * room(r)
        at = iota((count, 1), 0)
        expert = jnp.zeros((count, 1), jnp.int32)
        for k in range(1, slab):
            expert = expert + jnp.where(at >= k * room(r), 1, 0)
        within = at - expert * room(r) - part_of * CAP
        good = (within >= 0) & (within < CAP)
        return jnp.where(good, (z * slab + expert) * CAP + within, -1).astype(f32)

    def streams(r):
        if r == 0:
            return [(own_meta, None, tokens, 0)]
        taken = SENT[r - 1] * part
        return [(mz.at[way, r - 1], way, taken, 0 if r == 4 else way) for way in range(2)]

    def chosen(meta, taken, want, weighted):
        k0 = meta[0:1, 0:taken] * CAP + meta[1:2, 0:taken]
        k1 = meta[2:3, 0:taken] * CAP + meta[3:4, 0:taken]
        if not weighted:
            return ((k0 == want) | (k1 == want)).astype(bf16)
        return (
            jnp.where(k0 == want, meta[4:5, 0:taken], 0.0) + jnp.where(k1 == want, meta[5:6, 0:taken], 0.0)
        ).astype(bf16)

    def x_copy(r, d, src_place, dst_place, device):
        rows_of = pl.ds(pl.multiple_of(dst_place * room(r), 8), room(r))
        lands = pl.ds(pl.multiple_of(src_place * room(r), 8), room(r))
        n = ROUNDS.index(r)
        return remote(
            gb.at[n, rows_of, wing(d)],
            rb.at[n, lands, wing(d)],
            x_send.at[r % 4 and 1],
            x_recv.at[n],
            device,
        )

    def y_copy(r, s, src_place, dst_place, device):
        rows_of = pl.ds(pl.multiple_of(dst_place * room(r), 8), room(r))
        lands = pl.ds(pl.multiple_of(src_place * room(r), 8), room(r))
        n = ROUNDS.index(r)
        return remote(
            ob.at[n, rows_of, side(s)],
            yb.at[n, lands, side(s)],
            y_send.at[r % 4 and 1],
            y_recv.at[n, s],
            device,
        )

    def pick(r, d):
        n, count = ROUNDS.index(r), slab * room(r)
        known(r)
        for c in range(SENT[r - 1] if r else 0):
            arrived(r, c, d)
        picks = []
        for meta, way, taken, second in streams(r):
            picks.append((chosen(meta[...].astype(f32), taken, wanted(r, second), False), way, taken))

        @pl.loop(0, there // cols)
        def _(t):
            at = pl.ds(pl.multiple_of(d * there + t * cols, 128), cols)
            total = jnp.zeros((count, cols), f32)
            for one_hot, way, taken in picks:
                source = xn[0:taken, at] if way is None else dz[way, r - 1, 0:taken, at]
                total = total + dot(one_hot, source)
            gb[n, 0:count, at] = total.astype(bf16)

        for k in range(1, slab):
            place, device = slab_peer(k)
            go(x_copy(r, d, me, place, device))
        own = pl.ds(pl.multiple_of(me * room(r), 8), room(r))
        rb[n, own, wing(d)] = gb[n, own, wing(d)]

    def gate(r):
        n, count = ROUNDS.index(r), slab * room(r)
        if others:
            drained(rb.at[n, pl.ds(0, others * room(r))], x_recv.at[n])
        need(13, 14)
        rows = rb[n, 0:count, :]
        value = dot(rows, wg[...])
        hid[n, 0:count, :] = (value / (1.0 + jnp.exp(-value)) * dot(rows, wu[...])).astype(bf16)

    def give(r, s):
        n, count = ROUNDS.index(r), slab * room(r)
        need(15)
        hidden = hid[n, 0:count, :]

        @pl.loop(0, half // cols)
        def _(t):
            at = pl.ds(pl.multiple_of(s * half + t * cols, 128), cols)
            ob[n, 0:count, at] = dot(hidden, wd[:, at]).astype(bf16)

        for k in range(1, slab):
            place, device = slab_peer(k)
            go(y_copy(r, s, me, place, device))
        own = pl.ds(pl.multiple_of(me * room(r), 8), room(r))
        yb[n, own, side(s)] = ob[n, own, side(s)]

    def weigh(r, s):
        n, count = ROUNDS.index(r), slab * room(r)
        if others:
            drained(yb.at[n, pl.ds(0, others * room(r)), side(s)], y_recv.at[n, s])
        parts = []
        for meta, way, taken, second in streams(r):
            parts.append((chosen(meta[...].astype(f32), taken, wanted(r, second), True), way, taken))

        @pl.loop(0, half // cols)
        def _(t):
            at = pl.ds(pl.multiple_of(s * half + t * cols, 128), cols)
            for weights, way, taken in parts:
                value = dot_t(weights, yb[n, 0:count, at])
                if way is None:
                    acc[:, at] = value
                else:
                    ts[way, r - 1, 0:taken, at] = value.astype(bf16)

    def pass_on(h, c, s):
        if h < 4 and c < SENT[h]:
            drained(tr.at[:, h, chunk(c), side(s)], b_recv.at[1 + sum(SENT[1:h]) + c, s])
        for way, step in ways:
            if h < 4 and c < SENT[h]:
                at = slice(c * part, (c + 1) * part)
                ts[way, h - 1, at, side(s)] = (
                    ts[way, h - 1, at, side(s)].astype(f32) + tr[way, h, at, side(s)].astype(f32)
                ).astype(bf16)
            go(homeward(h, c, s, way, step))

    def finish(s):
        drained(tr.at[:, 0, :, side(s)], b_recv.at[0, s])

        @pl.loop(0, half // cols)
        def _(t):
            at = pl.ds(pl.multiple_of(s * half + t * cols, 128), cols)
            total = acc[:, at]
            for way in range(2):
                total = total + dot_t(perm[way], tr[way, 0, :, at])
            routed_ref[:, at] = total.astype(bf16)

        out = pltpu.make_async_copy(routed_ref.at[:, side(s)], routed_hbm.at[:, side(s)], w_sem.at[18 + s])
        out.start()
        leaving.append(out)

    leaving = []

    key_scale = size**-0.5

    def summary():
        need(6, 7, 8, 9, 10)
        gate = fg_ref[...]
        keep = jnp.minimum(gate, 0.0) - jnp.log1p(jnp.exp(-jnp.abs(gate))) + fb_ref[...]
        upto = (iota((span, span), 0) <= iota((span, span), 1)).astype(f32)
        total = jnp.dot(
            stacked([keep], span), upto, preferred_element_type=f32, precision=lax.Precision.HIGHEST
        )[0:1]
        lead = ig_ref[...] - total
        last = total[:, span - 1 : span]
        top = jnp.max(last + lead, axis=1, keepdims=True)
        spread = jnp.exp(last + lead - top) * key_scale
        unit = (iota((8, 8), 0) == iota((8, 8), 1)).astype(f32)
        columns = lax.dot_general(
            stacked([total, spread], span),
            unit,
            (((0,), (0,)), ((), ())),
            preferred_element_type=f32,
            precision=lax.Precision.HIGHEST,
        )
        bcol_s[...] = columns[:, 0:1]
        weighted = k_ref[...].astype(f32) * columns[:, 1:2]
        ct[...] = dot_t(weighted.astype(bf16), v_ref[...])
        normer = jnp.sum(weighted, axis=0, keepdims=True)
        wide = jnp.zeros((1, size), f32)
        sm[...] = stacked([normer, last + wide, top + wide], size)
        for k in range(1, slab):
            place, device = slab_peer(k)
            for copy in s_copies(me, place, device):
                go(copy)
        sl[me] = ct[pl.ds(pl.multiple_of(me * piece, 8), piece), :]
        sm_all[me] = sm[...]
        lead_s[...] = lead

    def s_copies(src_place, dst_place, device):
        return (
            remote(
                ct.at[pl.ds(pl.multiple_of(dst_place * piece, 8), piece)],
                sl.at[src_place],
                s_send.at[0],
                s_recv.at[0],
                device,
            ),
            remote(sm, sm_all.at[src_place], s_send.at[1], s_recv.at[1], device),
        )

    def local():
        need(5)
        lead = lead_s[...]
        block = min(128, span)
        for at in range(0, span, block):
            end = at + block
            q = q_ref[at:end, :]
            products = dot_nt(q, k_ref[0:end, :]) * key_scale
            decay = bcol_s[at:end, :] + lead[:, 0:end]
            decay = jnp.where(iota((block, end), 1) <= iota((block, end), 0) + at, decay, floor_log)
            peak = jnp.max(decay, axis=1, keepdims=True)
            scores = products * jnp.exp(decay - peak)
            lpeak_s[at:end, :] = peak
            den_s[at:end, :] = jnp.sum(scores, axis=1, keepdims=True)
            num_loc[at:end, :] = dot(scores.astype(bf16), v_ref[0:end, :])

    def t_copies(src_z, k):
        return (
            remote(zs_out, zt.at[src_z], t_send.at[0], t_recv.at[0], z_peer(k)),
            remote(zm_out, zm.at[src_z], t_send.at[1], t_recv.at[1], z_peer(k)),
        )

    def unpacked(meta, memory):
        return (meta[1:2, :], meta[2:3, :], memory, meta[0:1, :])

    def nothing():
        zero = jnp.zeros((1, size), f32)
        return (zero, zero + floor_log, jnp.zeros((piece, size), f32), zero)

    def inside():
        if others:
            drained(sl.at[pl.ds(0, others)], s_recv.at[0])
            drained(sm_all.at[pl.ds(0, others)], s_recv.at[1])
        state = nothing()
        for p in range(slab):
            ep_slice[p] = state[2]
            ep_meta[p] = stacked([state[3], state[0], state[1]], size)
            state = joined(state, unpacked(sm_all[p], sl[p]))
        zs_out[...] = state[2].astype(bf16)
        zm_out[...] = stacked([state[3], state[0], state[1]], size, 4)
        for k in (1, 7, 2, 6, 3, 5):
            arrived(min(k, NZ - k), 0, 0)
            for copy in t_copies(z, k):
                go(copy)

    def opposite_side():
        arrived(4, 0, 0)
        for copy in t_copies(z, 4):
            go(copy)

    def e_copy(src_place, dst_place, device):
        return remote(
            es.at[dst_place],
            ent.at[pl.ds(pl.multiple_of(src_place * piece, 16), piece)],
            e_send.at[0],
            e_recv.at[0],
            device,
        )

    def across():
        drained(zt.at[pl.ds(0, NZ - 1)], t_recv.at[0])
        drained(zm.at[pl.ds(0, NZ - 1)], t_recv.at[1])
        zt[z] = zs_out[...]
        zm[z] = zm_out[...]
        state = nothing()
        for s in range(NZ - 1):
            earlier = s < z
            total, peak, memory, normer = unpacked(zm[s], zt[s].astype(f32))
            part_of = (
                jnp.where(earlier, total, 0.0),
                jnp.where(earlier, peak, floor_log),
                jnp.where(earlier, memory, 0.0),
                jnp.where(earlier, normer, 0.0),
            )
            state = joined(state, part_of)
        for p in range(slab):
            es[p] = joined(state, unpacked(ep_meta[p], ep_slice[p]))[2].astype(bf16)
        for k in range(1, slab):
            place, device = slab_peer(k)
            go(e_copy(me, place, device))
        ent[pl.ds(pl.multiple_of(me * piece, 16), piece), :] = es[me]
        total, peak, _, normer = state
        both = joined((total, peak, None, normer), unpacked(ep_meta[me], None))
        into_s[...] = stacked([both[3], both[0], both[1]], size)

    def h_copy(src_y, dst_y, device):
        quarter = span // ny
        return remote(
            hs.at[pl.ds(pl.multiple_of(dst_y * quarter, 16), quarter)],
            hb.at[src_y],
            h_send.at[0],
            h_recv.at[0],
            device,
        )

    def cells():
        need(11)
        _, stabil, _, normer = unpacked(into_s[...], None)
        if others:
            drained(ent.at[pl.ds(0, others * piece)], e_recv.at[0])
        block = min(256, span)
        for at in range(0, span, block):
            end = at + block
            q = q_ref[at:end, :]
            carried = bcol_s[at:end, :] + stabil[:, 0:1]
            peak = jnp.maximum(carried, lpeak_s[at:end, :])
            factor = jnp.exp(lpeak_s[at:end, :] - peak)
            across_ = jnp.exp(carried - peak)
            den = factor * den_s[at:end, :] + across_ * jnp.sum(q.astype(f32) * normer, axis=1, keepdims=True)
            num = factor * num_loc[at:end, :] + across_ * dot(q, ent[...])
            cell = num / jnp.maximum(jnp.abs(den), jnp.exp(-peak))
            hs[at:end, :] = (cell * hscale_ref[...]).astype(bf16)
        quarter = span // ny
        for k in range(1, ny):
            place, device = y_peer(k)
            go(h_copy(yy, place, device))
        hb[yy] = hs[pl.ds(pl.multiple_of(yy * quarter, 16), quarter), :]

    def project():
        if ny > 1:
            drained(hb.at[pl.ds(0, ny - 1)], h_recv.at[0])
        need(12, 16)
        quarter = span // ny
        total = jnp.zeros((quarter, width), f32)
        for y in range(ny):
            total = total + dot(hb[y], wo[y * size : (y + 1) * size, :])
        squares = jnp.mean(total * total, axis=-1, keepdims=True)
        mixed_ref[...] = (total * lax.rsqrt(squares + norm_eps) * pscale_ref[...]).astype(bf16)
        out = pltpu.make_async_copy(mixed_ref, mixed_hbm, w_sem.at[17])
        out.start()
        leaving.append(out)

    steps = dict(
        S=send,
        pick=pick,
        gate=gate,
        give=give,
        weigh=weigh,
        P=pass_on,
        summary=summary,
        local=local,
        inside=inside,
        far=opposite_side,
        across=across,
        cells=cells,
        project=project,
        final=finish,
    )
    for line in ORDER.split():
        name, *numbers = line.split(",")
        steps[name](*(int(k) for k in numbers))
    drained(mz.at[:, pl.ds(0, 3)], meta_send.at[0])
    drained(mz.at[:, 3, :, pl.ds(0, min(tokens, 128))], meta_send.at[1])
    drained(dz.at[:, pl.ds(0, 3)], z_send.at[0])
    drained(tr.at[:, pl.ds(0, 3)], b_send.at[0])
    drained(zt.at[pl.ds(0, NZ - 1)], t_send.at[0])
    drained(zm.at[pl.ds(0, NZ - 1)], t_send.at[1])
    if others:
        for sems, held_in in ((x_send, gb), (y_send, yb)):
            drained(held_in.at[pl.ds(0, 2), pl.ds(0, others * room(0))], sems.at[0])
            drained(held_in.at[pl.ds(0, 3), pl.ds(0, others * room(1))], sems.at[1])
        drained(sl.at[pl.ds(0, others)], s_send.at[0])
        drained(sm_all.at[pl.ds(0, others)], s_send.at[1])
        drained(es.at[pl.ds(0, others)], e_send.at[0])
    if ny > 1:
        drained(hb.at[pl.ds(0, ny - 1)], h_send.at[0])
    for copy in leaving:
        copy.wait()


def copied(a_ref, b_ref, a_out, b_out, a_held, b_held, sems):
    moves = []
    for n, (src, held, dst) in enumerate(((a_ref, a_held, a_out), (b_ref, b_held, b_out))):
        block = src.shape[0] // 2
        for k in range(2):
            at = pl.ds(k * block, block)
            into = pltpu.make_async_copy(src.at[at], held.at[at], sems.at[n, k, 0])
            into.start()
            moves.append((into, pltpu.make_async_copy(held.at[at], dst.at[at], sems.at[n, k, 1])))
    for into, out in moves:
        into.wait()
        out.start()
    for _, out in moves:
        out.wait()


def shards(
    memory_query_matrix,
    memory_key_matrix,
    memory_value_matrix,
    input_gate_logits,
    forget_gate_logits,
    forget_log_boosts,
    head_norm_scale,
    memory_output_matrix,
    projection_norm_scale,
    second_batch_rows,
    expert_prenorm_scale,
    selected_expert_index,
    group_route_probability,
    expert_choice_scores,
    expert_gate_matrix,
    expert_up_matrix,
    expert_down_matrix,
):
    nx, nc, ny = (lax.axis_size(a) for a in ("ep_1", "ep_2", "tp"))
    slab = nx * nc
    tokens, width = second_batch_rows.shape
    span, size = memory_query_matrix.shape
    hidden = expert_gate_matrix.shape[2]
    piece = size // slab
    part = tokens // 4
    cellw = memory_output_matrix.shape[0]
    most = slab * 2 * CAP
    anywhere = pl.BlockSpec(memory_space=pl.ANY)
    dma = pltpu.SemaphoreType.DMA
    rounds = len(ROUNDS)
    inputs = (
        second_batch_rows,
        selected_expert_index.T,
        group_route_probability[None, :],
        expert_choice_scores.T,
        expert_prenorm_scale[None, :],
        memory_query_matrix,
        memory_key_matrix,
        memory_value_matrix,
        input_gate_logits,
        forget_gate_logits,
        forget_log_boosts,
        head_norm_scale[None, :],
        projection_norm_scale[None, :],
        expert_gate_matrix,
        expert_up_matrix,
        expert_down_matrix,
        memory_output_matrix,
    )
    scratch = [pltpu.VMEM(a.shape[-2:], a.dtype) for a in inputs]
    scratch += [
        pltpu.VMEM((tokens, width), bf16),
        pltpu.VMEM((span // ny, width), bf16),
        pltpu.VMEM((tokens, width), bf16),
        pltpu.VMEM((rounds, most, hidden), bf16),
        pltpu.VMEM((1, span), f32),
        pltpu.VMEM((8, size), f32),
        pltpu.VMEM((2, tokens, width), bf16),
        pltpu.VMEM((2, tokens, tokens), bf16),
        pltpu.VMEM((8, tokens), f32),
        pltpu.VMEM((2, 8, tokens), bf16),
        pltpu.VMEM((2, 4, 8, tokens), bf16),
        pltpu.VMEM((2, 4, tokens, width), bf16),
        pltpu.VMEM((rounds, most, width), bf16),
        pltpu.VMEM((rounds, most, width), bf16),
        pltpu.VMEM((rounds, most, width), bf16),
        pltpu.VMEM((rounds, most, width), bf16),
        pltpu.VMEM((2, 4, tokens, width), bf16),
        pltpu.VMEM((2, 4, tokens, width), bf16),
        pltpu.VMEM((tokens, width), f32),
        pltpu.VMEM((size, size), f32),
        pltpu.VMEM((8, size), f32),
        pltpu.VMEM((slab, piece, size), f32),
        pltpu.VMEM((slab, 8, size), f32),
        pltpu.VMEM((piece, size), bf16),
        pltpu.VMEM((4, size), f32),
        pltpu.VMEM((NZ, piece, size), bf16),
        pltpu.VMEM((NZ, 4, size), f32),
        pltpu.VMEM((slab, piece, size), f32),
        pltpu.VMEM((slab, 8, size), f32),
        pltpu.VMEM((slab, piece, size), bf16),
        pltpu.VMEM((size, size), bf16),
        pltpu.VMEM((span, size), f32),
        pltpu.VMEM((span, 1), f32),
        pltpu.VMEM((span, 1), f32),
        pltpu.VMEM((span, 1), f32),
        pltpu.VMEM((span, size), bf16),
        pltpu.VMEM((ny, span // ny, size), bf16),
        dma((18 + HALVES,)),
        dma((2,)),
        dma((4,)),
        dma((1,)),
        dma((sum(SENT), WINGS)),
        dma((1,)),
        dma((1 + sum(SENT[1:]), HALVES)),
        dma((2,)),
        dma((rounds,)),
        dma((2,)),
        dma((rounds, HALVES)),
        dma((2,)),
        dma((2,)),
        dma((2,)),
        dma((2,)),
        dma((1,)),
        dma((1,)),
        dma((1,)),
        dma((1,)),
    ]
    shapes = (
        jax.ShapeDtypeStruct((span // ny, width), bf16),
        jax.ShapeDtypeStruct((tokens, width), bf16),
    )
    mixed, routed = pl.pallas_call(
        functools.partial(body, (nx, nc, ny)),
        out_shape=shapes,
        in_specs=[anywhere] * len(inputs),
        out_specs=(anywhere, anywhere),
        scratch_shapes=scratch,
        compiler_params=pltpu.CompilerParams(
            collective_id=0, has_side_effects=True, vmem_limit_bytes=67043328
        ),
    )(*inputs)
    return pl.pallas_call(
        copied,
        out_shape=shapes,
        in_specs=[anywhere] * 2,
        out_specs=(anywhere, anywhere),
        scratch_shapes=[
            pltpu.VMEM(shapes[0].shape, bf16),
            pltpu.VMEM(shapes[1].shape, bf16),
            dma((2, 2, 2)),
        ],
    )(mixed, routed)


def solution(mesh):
    finer = Mesh(mesh.devices.reshape(8, 4, 2, mesh.shape["tp"]), EP_TP)
    in_specs = (
        P(EP, "tp"),
        P(EP, "tp"),
        P(EP, "tp"),
        P("tp", EP),
        P("tp", EP),
        P("tp", EP),
        P("tp"),
        P(),
        P(),
        P(EP_TP, None),
        P(),
        P(EP_TP, None),
        P(EP_TP),
        P(EP_TP, None),
        P(EP, None, None),
        P(EP, None, None),
        P(EP, None, None),
    )
    out_specs = (P(EP_TP, None), P(EP_TP, None))
    return jax.shard_map(shards, mesh=finer, in_specs=in_specs, out_specs=out_specs, check_vma=False)
```
